128 devices in a mesh: tp: 16 (over z, y), dp: 8 (over x, core).
Axes of the slice: x: 4, y: 4, z: 4, core: 2. Of those that a mesh axis runs over, the one named last changes fastest.
Arguments:
- activation_rows: bfloat16 [2048, 4096], P(None, 'dp'), may hold values from -24 to 24
- fresh_spans: int32 [256], P('dp'), may hold values from 1 to 8, 768 in all
- entry_rescale_vector: float32 [2, 4096], P(None, 'dp'), may hold values from 0.1 to 1.9
- probe_kernel: bfloat16 [2, 4096, 4096], P(None, 'dp', 'tp'), may hold values from -0.09375 to 0.09375
- retention_kernel: bfloat16 [2, 4096, 4096], P(None, 'dp', 'tp'), may hold values from -0.09375 to 0.09375
- content_kernel: bfloat16 [2, 4096, 4096], P(None, 'dp', 'tp'), may hold values from -0.09375 to 0.09375
- valve_kernel: bfloat16 [2, 4096, 4096], P(None, 'dp', 'tp'), may hold values from -0.09375 to 0.09375
- retention_minimum: float32 [2, 4096], P(None, 'tp'), may hold values from 0 to 0.99
- extra_attenuation: float32 [2, 2048, 32], P(None, 'dp', 'tp'), may hold values from -0.7 to 0
- channel_rescale_vector: float32 [2, 4096], P(None, 'tp'), may hold values from 0.1 to 1.9
- emission_kernel: bfloat16 [2, 4096, 4096], P(None, 'tp', 'dp'), may hold values from -0.09375 to 0.09375
- memory_grids: float32 [2, 256, 32, 128, 128], P(None, 'dp', 'tp'), may hold values from -0.6 to 0.6
Outputs:
- mixed: bfloat16 [2048, 4096], P(None, 'dp')
- new_states: float32 [2, 256, 32, 128, 128], P(None, 'dp', 'tp')
The draws below stay inside these ranges and needn't reach their ends.
Inputs may be any that keep to these rules, and one draw needn't show every extreme that they name: `fresh_spans`: each sequence has at least one live slot.
All inputs are finite; a program needn't handle non-finite values. No bound on the sum of `fresh_spans` on one device may be relied on, other than what follows from the above.
Results may differ from the reference program's by a relative error of at most 0.017.
Values may be sent and summed in bfloat16 or wider, within the bound.
A program may use at most 128 MiB of HBM per device.

```python
import math
import jax
import jax.numpy as jnp
import numpy as np
from jax import lax

D = 4096
HEADS = 32
DK = 128
DV = 128
NEW = 8
BLOCKS = 2
SEQS = 256
ROWS = 2048
HK = 4096
HV = 4096
N_DP = 8


def draw_activation_rows(key, part):
    column_scale = jnp.exp(jnp.linspace(0.0, math.log(4.0), D, dtype=jnp.float32))[None, :]
    base = jnp.clip(jax.random.normal(key, (ROWS, D), jnp.float32), -6.0, 6.0)
    return jnp.clip(base * column_scale, -24.0, 24.0).astype(jnp.bfloat16)


def draw_extra_attenuation(key, part):
    hits = jax.random.randint(jax.random.fold_in(key, 3), (BLOCKS, ROWS, HEADS), 0, 10) == 0
    depth = jax.random.uniform(jax.random.fold_in(key, 4), (BLOCKS, ROWS, HEADS), jnp.float32, math.log(0.5), math.log(0.8))
    return jnp.where(hits, depth, jnp.zeros_like(depth)).astype(jnp.float32)


def levels(stream_key, dims, cuts, smallest, high):
    factor_of = 1.0
    for position, parts in cuts:
        heights = jax.random.uniform(jax.random.fold_in(jax.random.fold_in(stream_key, 6), position), (parts,), jnp.float32, smallest / len(cuts), high / len(cuts))
        factor_of = factor_of * jnp.repeat(jnp.exp(heights), dims[position] // parts).reshape((-1,) + (1,) * (len(dims) - 1 - position))
    return factor_of


def length_profile(count, total, most, skew):
    loads = [(1 << 20) // math.isqrt(standing ** skew) + 1 for standing in range(2, count + 1)]
    surplus, holding = total - most - (count - 1), [1] * (count - 1)
    while surplus > 0:
        candidates = [i for i in range(count - 1) if holding[i] < most]
        mass, left = sum([loads[i] for i in candidates]), surplus
        for i in candidates:
            more = min(most - holding[i], max(1, left * loads[i] // mass), surplus)
            holding[i] = holding[i] + more
            surplus = surplus - more
    return np.array([most] + holding)


def ragged(stream_key, count, total, reach, skew):
    if count == 2:
        one = jax.random.randint(stream_key, (), max(1, total - reach), min(reach, total - 1) + 1)
        return jnp.stack([one, total - one])
    tallies = jnp.asarray(length_profile(count, total, reach, skew), jnp.int32)
    twos = (count - 1) // 2
    giver, receiver = tallies[1:1 + 2 * twos:2], tallies[2:2 + 2 * twos:2]
    room = jnp.minimum(giver - 1, reach - receiver)
    passed = jax.random.randint(jax.random.fold_in(stream_key, 1), (twos,), 0, 1 << 20) % (room + 1)
    tallies = tallies.at[1:1 + 2 * twos:2].set(giver - passed).at[2:2 + 2 * twos:2].set(receiver + passed)
    return tallies[jax.random.permutation(jax.random.fold_in(stream_key, 2), count)]


def noise(rng, dims, scale, most, split=(), kind=jnp.bfloat16):
    result = jax.random.normal(rng, dims, jnp.float32) * scale
    if len(split) > 0:
        result = levels(rng, dims, split, -0.22, 0.18) * result
    return jnp.clip(result, min=-most, max=most).astype(kind)


def setup_inputs(seed: int = 0) -> dict:
    splits = jax.random.split(jax.random.key(seed), 13)
    return {
        "activation_rows": draw_activation_rows(jax.random.fold_in(splits[12], 71), 0),
        "fresh_spans": ragged(splits[1], SEQS, 3 * SEQS, NEW, 2).astype(jnp.int32),
        "entry_rescale_vector": jnp.clip(1.0 + 0.18 * jax.random.normal(splits[2], (BLOCKS, D), jnp.float32), 0.1, 1.9),
        "probe_kernel": noise(splits[3], (BLOCKS, D, HK), D ** -0.5, 0.09375, ((1, 8), (2, 16))),
        "retention_kernel": noise(splits[4], (BLOCKS, D, HK), D ** -0.5, 0.09375, ((1, 8), (2, 16))),
        "content_kernel": noise(splits[5], (BLOCKS, D, HV), D ** -0.5, 0.09375, ((1, 8), (2, 16))),
        "valve_kernel": noise(splits[6], (BLOCKS, D, HV), D ** -0.5, 0.09375, ((1, 8), (2, 16))),
        "retention_minimum": jnp.clip(0.99 * jax.random.uniform(splits[7], (BLOCKS, HK), jnp.float32) ** levels(splits[7], (BLOCKS, HK), ((1, 16),), -0.2, 0.2), 0.0, 0.99),
        "extra_attenuation": draw_extra_attenuation(jax.random.fold_in(splits[12], 71), 0),
        "channel_rescale_vector": jnp.clip(1.0 + 0.18 * jax.random.normal(splits[9], (BLOCKS, HV), jnp.float32), 0.1, 1.9),
        "emission_kernel": noise(splits[10], (BLOCKS, HV, D), HV ** -0.5, 0.09375, ((1, 16), (2, 8))),
        "memory_grids": noise(splits[11], (BLOCKS, SEQS, HEADS, DK, DV), 0.1, 0.6, ((1, 8), (2, 16)), jnp.float32),
    }


EPSILON = 1e-05

def update_tick(probe_scores, retention_scores, content_scores, valve_scores, minimum_bound, spike_ledger, attention_multiplier, stream_spans, memory_grid):
    stream_tally = memory_grid.shape[0]
    attention_tally = memory_grid.shape[1]
    key_dim = memory_grid.shape[2]
    value_dim = memory_grid.shape[3]
    position_tally = probe_scores.shape[0] // stream_tally

    def split_heads(array, width):
        return array.astype(jnp.float32).reshape(stream_tally, position_tally, attention_tally, width)
    queries = jax.nn.silu(split_heads(probe_scores, key_dim))
    forget_in = split_heads(retention_scores, key_dim)
    lower_heads = minimum_bound.reshape(attention_tally, key_dim)
    retention_sigmoid = lower_heads + (1.0 - lower_heads) * jax.nn.sigmoid(forget_in)
    key_vecs = (1.0 - lower_heads) * jax.nn.sigmoid(-forget_in)
    log_attenuation = jnp.log(retention_sigmoid) + spike_ledger.reshape(stream_tally, position_tally, attention_tally)[..., None]
    values = split_heads(content_scores, value_dim)
    positions = lax.broadcasted_iota(jnp.int32, (stream_tally, position_tally), 1)
    live_mask = positions < stream_spans[:, None].astype(jnp.int32)

    def advance(matrix, inputs):
        query_now, key_now, decay_now, value_now, live_now = inputs
        updated = jnp.exp(decay_now)[..., None] * matrix + key_now[..., None] * value_now[..., None, :]
        matrix = jnp.where(live_now[:, None, None, None], updated, matrix)
        readout = jnp.einsum('shkv,shk->shv', matrix, query_now, precision=lax.Precision.HIGHEST)
        return (matrix, readout)
    ending_emission, readouts = lax.scan(advance, memory_grid, (jnp.moveaxis(queries, 1, 0), jnp.moveaxis(key_vecs, 1, 0), jnp.moveaxis(log_attenuation, 1, 0), jnp.moveaxis(values, 1, 0), jnp.moveaxis(live_mask, 1, 0)))
    readouts = jnp.moveaxis(readouts, 0, 1)
    normed = readouts * lax.rsqrt(lax.optimization_barrier(jnp.mean(readouts * readouts, axis=-1, keepdims=True)) + EPSILON)
    normed = normed * attention_multiplier.reshape(attention_tally, value_dim) * jax.nn.silu(split_heads(valve_scores, value_dim))
    normed = normed * live_mask.astype(jnp.float32)[..., None, None]
    return (normed.reshape(stream_tally * position_tally, attention_tally * value_dim).astype(jnp.bfloat16), ending_emission)

def blocked_product(normed, weight):
    width = D // N_DP
    total = jnp.zeros((normed.shape[0], weight.shape[1]), jnp.float32)
    for index in range(N_DP):
        partial_value = jnp.dot(normed[:, index * width:(index + 1) * width], weight[index * width:(index + 1) * width], preferred_element_type=jnp.float32)
        rounded = lax.optimization_barrier(partial_value.astype(jnp.bfloat16))
        total = total + rounded.astype(jnp.float32)
    return total

def reference(activation_rows, fresh_spans, entry_rescale_vector, probe_kernel, retention_kernel, content_kernel, valve_kernel, retention_minimum, extra_attenuation, channel_rescale_vector, emission_kernel, memory_grids):
    residual = activation_rows
    finals = []
    for layer_index in range(BLOCKS):
        current = residual.astype(jnp.float32)
        row_scale = lax.rsqrt(lax.optimization_barrier(jnp.mean(current * current, axis=1)) + EPSILON)
        normed = (current * entry_rescale_vector[layer_index]).astype(jnp.bfloat16)
        mapped_activation = [(blocked_product(normed, weight[layer_index]) * row_scale[:, None]).astype(jnp.bfloat16) for weight in (probe_kernel, retention_kernel, content_kernel, valve_kernel)]
        attention_yields, ending_emission = update_tick(mapped_activation[0], mapped_activation[1], mapped_activation[2], mapped_activation[3], retention_minimum[layer_index], extra_attenuation[layer_index], channel_rescale_vector[layer_index], fresh_spans, memory_grids[layer_index])
        finals.append(ending_emission)
        update = jnp.dot(attention_yields, emission_kernel[layer_index], preferred_element_type=jnp.float32).astype(jnp.bfloat16)
        residual = (current + update.astype(jnp.float32)).astype(jnp.bfloat16)
    return (residual, jnp.stack(finals))
```

```python
import functools

import jax
import jax.numpy as jnp
from jax import lax
from jax.experimental import pallas as pl
from jax.experimental.pallas import tpu as pltpu
from jax.sharding import PartitionSpec as P

D = 4096
BLOCKS = 2
EPSILON = 1e-05
RING = 4
SHARDS = 8
SEQS = 32
SLOTS = 8
SHARD_ROWS = SEQS * SLOTS
FEATURES = 512
CHANNELS = 256
HEADS = 2
LANES = 128
MESH = pl.DeviceIdType.MESH
F32 = jnp.float32
BF16 = jnp.bfloat16
VMEM_BYTES = 62 * 1024 * 1024


def here():
    dp, tp = lax.axis_index("dp"), lax.axis_index("tp")
    return lax.div(dp, 2), lax.rem(dp, 2), lax.div(tp, RING), lax.rem(tp, RING)


def device(x, core, z, y):
    return {"tp": z * RING + y, "dp": x * 2 + core}


def around(index, offset):
    return lax.rem(index + offset, RING)


def greet(peers):
    barrier = pltpu.get_barrier_semaphore()
    for peer in peers:
        pl.semaphore_signal(barrier, inc=1, device_id=peer, device_id_type=MESH)
    pl.semaphore_wait(barrier, len(peers))


def iota(shape, dim):
    return lax.broadcasted_iota(jnp.int32, shape, dim)


def dot(a, b):
    return jnp.dot(a, b, preferred_element_type=F32)


def dot_rows(a, b):
    return lax.dot_general(a, b, (((0,), (0,)), ((), ())), preferred_element_type=F32)


def chosen(rank_row, first, count):
    wanted = (iota((count, rank_row.shape[1]), 0) + first).astype(F32)
    return jnp.where(wanted == rank_row, 1.0, 0.0).astype(BF16)


def tables_kernel(spans, rank, column, gathered, send_sems, recv_sems):
    dp, tp = lax.axis_index("dp"), lax.axis_index("tp")
    others = [{"tp": tp, "dp": lax.rem(dp + offset, SHARDS)} for offset in range(1, SHARDS)]
    greet(others)
    copies = []
    for number, other in enumerate(others):
        copy = pltpu.make_async_remote_copy(
            spans,
            gathered.at[dp],
            send_sems.at[number],
            recv_sems.at[number],
            device_id=other,
            device_id_type=MESH,
        )
        copy.start()
        copies.append(copy)
    gathered[dp] = spans[...]

    own = spans[...].astype(F32)
    lane, row = iota((SEQS, SEQS), 1), iota((SEQS, SEQS), 0)
    before = jnp.sum(jnp.where(lane < row, own, 0.0), axis=1, keepdims=True)
    same = jnp.sum(jnp.where(lane == row, own, 0.0), axis=1, keepdims=True)
    column[0:SEQS, :] = jnp.broadcast_to(before, (SEQS, LANES))
    column[SEQS:, :] = jnp.broadcast_to(same, (SEQS, LANES))

    for copy in copies:
        copy.wait_recv()
    spans_all = jnp.concatenate([gathered[index] for index in range(SHARDS)], axis=0)
    spans_all = spans_all.astype(F32).astype(BF16)
    slot_index = iota((SEQS, SHARD_ROWS), 1)
    sequence = iota((SEQS, SHARD_ROWS), 0)
    for order in range(2):
        if order == 0:
            owner, position = lax.shift_right_logical(slot_index, 3), slot_index & 7
        else:
            owner, position = slot_index & 31, lax.shift_right_logical(slot_index, 5)
        earlier = jnp.where(sequence < owner, 1.0, 0.0).astype(BF16)
        equal = jnp.where(sequence == owner, 1.0, 0.0).astype(BF16)
        start, length = dot(spans_all, earlier), dot(spans_all, equal)
        place = position[0:SHARDS].astype(F32)
        ranks = jnp.where(place < length, start + place, -1.0)
        for index in range(SHARDS):
            rank[order * SHARDS + index] = ranks[index : index + 1]
    for copy in copies:
        copy.wait_send()


def tables(spans):
    return pl.pallas_call(
        tables_kernel,
        out_shape=(
            jax.ShapeDtypeStruct((2 * SHARDS, 1, SHARD_ROWS), F32),
            jax.ShapeDtypeStruct((2 * SEQS, LANES), F32),
        ),
        in_specs=[pl.BlockSpec(memory_space=pltpu.VMEM)],
        out_specs=(pl.BlockSpec(memory_space=pltpu.VMEM),) * 2,
        scratch_shapes=[
            pltpu.VMEM((SHARDS, 1, SEQS), jnp.int32),
            pltpu.SemaphoreType.DMA((SHARDS - 1,)),
            pltpu.SemaphoreType.DMA((SHARDS - 1,)),
        ],
        compiler_params=pltpu.CompilerParams(collective_id=0, has_side_effects=True),
        name="live_tables",
    )(spans)


def silu(a):
    return a * jax.nn.sigmoid(a)


def gates(b, hi, refs):
    spread, column, minimum, extra, q_decayed, own_read, keys, decay_total = refs

    def group(g, carry):
        start = column[pl.ds(pl.multiple_of(g * 8, 8), 8), :]
        span = column[pl.ds(pl.multiple_of(SEQS + g * 8, 8), 8), :]
        for head in range(HEADS):
            low, high = head * LANES, (head + 1) * LANES
            floor = minimum[b : b + 1, low:high]
            kept, values = [], []
            running = None
            for p in range(SLOTS):
                rows = pl.ds(pl.multiple_of(p * SEQS + g * 8, 8), 8)
                q = silu(spread[b, head, rows, :])
                f = spread[b, HEADS + head, rows, :]
                v = spread[b, 2 * HEADS + head, rows, :]
                added = jnp.exp(extra[b, pl.ds(g * 64 + p, 8, stride=8), :])[:, head : head + 1]
                live = jnp.logical_and(span > p, start + p < hi)
                forget = floor + (1.0 - floor) * jax.nn.sigmoid(f)
                decay = jnp.where(live, forget * added, 1.0)
                key = jnp.where(live, (1.0 - floor) * jax.nn.sigmoid(-f), 0.0)
                running = decay if p == 0 else running * decay
                kept = [old * decay for old in kept] + [key]
                values.append(v)
                read = None
                for old, value in zip(kept, values):
                    term = jnp.sum(q * old, axis=1, keepdims=True) * value
                    read = term if read is None else read + term
                q_decayed[head, rows, :] = q * running
                own_read[head, rows, :] = read
            for p in range(SLOTS):
                rows = pl.ds(pl.multiple_of(p * SEQS + g * 8, 8), 8)
                keys[b, head, rows, :] = kept[p]
            decay_total[b, pl.ds(pl.multiple_of(g * 8, 8), 8), low:high] = running
        return carry

    lax.fori_loop(0, SEQS // 8, group, 0)


def reads(b, refs):
    spread, states, gain, q_decayed, own_read, heads_out = refs
    together = 4

    def group(g, carry):
        for unit in range(together):
            s = g * together + unit
            rows = pl.ds(s, SLOTS, stride=SEQS)
            for head in range(HEADS):
                low, high = head * LANES, (head + 1) * LANES
                read = dot(q_decayed[head, rows, :].astype(BF16), states[b, s, head].astype(BF16))
                read = read + own_read[head, rows, :]
                square = jnp.mean(read * read, axis=1, keepdims=True)
                gate = silu(spread[b, 3 * HEADS + head, rows, :])
                out = read * lax.rsqrt(square + EPSILON) * gain[b : b + 1, low:high] * gate
                heads_out[pl.ds(pl.multiple_of(s * SLOTS, SLOTS), SLOTS), low:high] = out
        return carry

    lax.fori_loop(0, SEQS // together, group, 0)


def blocks_kernel(pieces, *refs):
    count = len(pieces)
    (act, rank, column, gain_in, w_q, w_f, w_v, w_g, minimum, extra, gain_out, emission, memory) = refs[:13]
    (out_x, out_keys, out_values, out_decay) = refs[13:17]
    refs = list(refs[17:])

    def take(number):
        taken = refs[:number]
        del refs[:number]
        return taken

    (raw, gain_peer, weights, outward, states, normed, spread, q_decayed, own_read, heads_out, added_wide, keys, decay_total) = take(13)
    (final_x, local_sems, swap_send, swap_recv, send_sems, recv_sems) = take(6)
    per = [take(13) for _ in range(count)]
    x, core, z, y = here()
    dp = x * 2 + core

    xs = [device(around(x, o), core, z, y) for o in range(1, RING)]
    ys = [device(x, core, z, around(y, o)) for o in range(1, RING)]
    zs = [device(x, core, around(z, o), y) for o in range(1, RING)]
    crossed = [device(x, 1 - core, around(z, o), y) for o in range(RING)]
    partner = crossed[0]
    kernels = (w_q, w_f, w_v, w_g)

    local, swaps, sent = [], [], []

    def bring(source, target):
        copy = pltpu.make_async_copy(source, target, local_sems.at[len(local)])
        copy.start()
        local.append(copy)
        return copy

    def swap(source, target):
        number = len(swaps)
        copy = pltpu.make_async_remote_copy(
            source,
            target,
            swap_send.at[number],
            swap_recv.at[number],
            device_id=partner,
            device_id_type=MESH,
        )
        copy.start()
        swaps.append(copy)
        return copy

    def send(b, i, phase, number, source, target, peer):
        copy = pltpu.make_async_remote_copy(
            source,
            target,
            send_sems.at[b, i, phase, number],
            recv_sems.at[b, i, phase, number],
            device_id=peer,
            device_id_type=MESH,
        )
        copy.start()
        sent.append(copy)
        return copy

    own_rows = [
        bring(act.at[pl.ds((j * 2 + core) * SHARD_ROWS, SHARD_ROWS), :], raw.at[j, :, 0:FEATURES])
        for j in range(RING)
    ]
    own_weights = [
        [bring(kernels[k].at[b], weights.at[b, 0:FEATURES, k * CHANNELS : (k + 1) * CHANNELS]) for k in range(4)]
        for b in range(BLOCKS)
    ]
    own_outward = [bring(emission.at[b], outward.at[b, :, 0:FEATURES]) for b in range(BLOCKS)]
    own_states = [bring(memory.at[b], states.at[b]) for b in range(BLOCKS)]

    greet(xs + ys + zs + crossed)

    peer_rows = [
        swap(
            act.at[pl.ds((j * 2 + 1 - core) * SHARD_ROWS, SHARD_ROWS), :],
            raw.at[j, :, FEATURES : 2 * FEATURES],
        )
        for j in range(RING)
    ]
    peer_gain = swap(gain_in, gain_peer)
    peer_weights, peer_outward = [], []
    for b in range(BLOCKS):
        peer_weights.append(
            [
                swap(
                    kernels[k].at[b],
                    weights.at[b, FEATURES : 2 * FEATURES, k * CHANNELS : (k + 1) * CHANNELS],
                )
                for k in range(4)
            ]
        )
        peer_outward.append(swap(emission.at[b], outward.at[b, :, FEATURES : 2 * FEATURES]))

    for j in range(RING):
        own_rows[j].wait()
        peer_rows[j].wait_recv()
        for i, (first, rows) in enumerate(pieces):
            picked = dot(chosen(rank[j * 2 + core], first, rows), raw[j]).astype(BF16)
            per[i][0][0, j] = picked[:, 0:FEATURES]
            per[i][1][0, j] = picked[:, FEATURES:]
    peer_gain.wait_recv()
    for b in range(BLOCKS):
        added_wide[b, :, 0:HEADS] = extra[b]

    outgoing = []

    def piece_steps(i):
        first, rows = pieces[i]
        (x_own, x_peer, parts, got, squares, got_squares, heads, u_own, u_peer, one, two_own, two_peer, last_peer) = per[i]
        for b in range(BLOCKS):
            eye = iota((rows, LANES), 0) == iota((rows, LANES), 1)
            for j in range(RING):
                a = x_own[b, j].astype(F32)
                c = x_peer[b, j].astype(F32)
                total = jnp.sum(a * a, axis=1, keepdims=True) + jnp.sum(c * c, axis=1, keepdims=True)
                squares[b, j] = jnp.sum(jnp.where(eye, total, 0.0), axis=0, keepdims=True)
                normed[j * rows : (j + 1) * rows, 0:FEATURES] = (a * gain_in[b : b + 1]).astype(BF16)
                normed[j * rows : (j + 1) * rows, FEATURES:] = (c * gain_peer[b : b + 1]).astype(BF16)
            waits = []
            for o in (2, 1, 3):
                waits.append(
                    send(b, i, 1, o - 1, squares.at[b, around(x, o)], got_squares.at[b, o - 1], xs[o - 1])
                )
            if i == 0:
                for k in range(4):
                    own_weights[b][k].wait()
                    peer_weights[b][k].wait_recv()

            def project(k, carry, b=b):
                columns = pl.ds(pl.multiple_of(k * CHANNELS, CHANNELS), CHANNELS)
                product = dot(normed[0 : RING * rows], weights[b, :, columns]).astype(BF16)
                for j in range(RING):
                    parts[b, j, :, columns] = product[j * rows : (j + 1) * rows]
                return carry

            lax.fori_loop(0, 4, project, 0)
            for o in (2, 1, 3):
                waits.append(send(b, i, 0, o - 1, parts.at[b, around(x, o)], got.at[b, o - 1], xs[o - 1]))
            yield

            for wait in waits:
                wait.wait_recv()
            square = squares[b, x] + got_squares[b, 0] + got_squares[b, 1] + got_squares[b, 2]
            scale_row = lax.rsqrt(square / D + EPSILON)
            scale = jnp.sum(jnp.where(eye, scale_row, 0.0), axis=1, keepdims=True)
            places = chosen(rank[SHARDS + dp], first, rows)

            def expand(k, carry, b=b, scale=scale, places=places):
                columns = pl.ds(pl.multiple_of(k * CHANNELS, CHANNELS), CHANNELS)
                total = parts[b, x, :, columns].astype(F32)
                for o in range(RING - 1):
                    total = total + got[b, o, :, columns].astype(F32)
                placed = dot_rows(places, (total * scale).astype(BF16))
                for head in range(HEADS):
                    part = placed[:, head * LANES : (head + 1) * LANES]
                    if i > 0:
                        part = part + spread[b, k * HEADS + head]
                    spread[b, k * HEADS + head] = part
                return carry

            lax.fori_loop(0, 4, expand, 0)
            gates(b, first + rows, (spread, column, minimum, added_wide, q_decayed, own_read, keys, decay_total))
            if i == 0:
                own_states[b].wait()
            reads(b, (spread, states, gain_out, q_decayed, own_read, heads_out))
            heads[b, x] = dot(chosen(rank[dp], first, rows), heads_out[...].astype(BF16)).astype(BF16)
            waits = [send(b, i, 2, o - 1, heads.at[b, x], heads.at[b, x], xs[o - 1]) for o in (2, 1, 3)]
            if i == count - 1:
                for source, target in (
                    (keys.at[b], out_keys.at[b]),
                    (spread.at[b, 2 * HEADS : 3 * HEADS], out_values.at[b]),
                    (decay_total.at[b], out_decay.at[b]),
                ):
                    outgoing.append(bring(source, target))
            if i == 0:
                own_outward[b].wait()
                peer_outward[b].wait_recv()
            yield

            for wait in waits:
                wait.wait_recv()
            all_heads = heads[b].reshape(RING * rows, CHANNELS)
            for half, target in enumerate((u_own, u_peer)):
                for part in range(2):
                    low = part * CHANNELS
                    columns = slice(half * FEATURES + low, half * FEATURES + low + CHANNELS)
                    product = dot(all_heads, outward[b, :, columns]).astype(BF16)
                    for j in range(RING):
                        target[b, j, :, low : low + CHANNELS] = product[j * rows : (j + 1) * rows]
            waits = []
            for o in (2, 1, 3):
                waits.append(send(b, i, 3, o - 1, u_own.at[b, around(y, o)], one.at[b, 0, o - 1], ys[o - 1]))
                waits.append(send(b, i, 4, o - 1, u_peer.at[b, around(z, o)], one.at[b, 1, o - 1], zs[o - 1]))
            yield

            for wait in waits:
                wait.wait_recv()
            waits = []
            for half, (mine, at, slots, own, peers) in enumerate(
                ((u_own, y, two_own, z, zs), (u_peer, z, two_peer, y, ys))
            ):
                total = mine[b, at].astype(F32)
                for o in range(RING - 1):
                    total = total + one[b, half, o].astype(F32)
                slots[b, own] = total.astype(BF16)
                for o in (2, 1, 3):
                    waits.append(send(b, i, 5 + half, o - 1, slots.at[b, own], slots.at[b, own], peers[o - 1]))
            yield

            for wait in waits:
                wait.wait_recv()
            waits = []
            for half, (slots, old, at) in enumerate(((two_own, x_own, y), (two_peer, x_peer, z))):
                total = slots[b, 0].astype(F32)
                for o in range(1, RING):
                    total = total + slots[b, o].astype(F32)
                fresh = (old[b, at].astype(F32) + total.astype(BF16).astype(F32)).astype(BF16)
                if b < BLOCKS - 1:
                    old[b + 1, at] = fresh
                    peers = ys if half == 0 else zs
                    for o in (2, 1, 3):
                        waits.append(send(b, i, 7 + half, o - 1, old.at[b + 1, at], old.at[b + 1, at], peers[o - 1]))
                elif half == 0:
                    place = final_x.at[core, y, first : first + rows]
                    final_x[core, y, first : first + rows] = fresh
                    for o in (2, 1, 3):
                        waits.append(send(b, i, 7, o - 1, place, place, ys[o - 1]))
                else:
                    last_peer[...] = fresh
                    place = final_x.at[core, z, first : first + rows]
                    for o in (2, 1, 3, 0):
                        waits.append(send(b, i, 8, o, last_peer, place, crossed[o]))
            yield
            for wait in waits:
                wait.wait_recv()

    running = [piece_steps(i) for i in range(count)]
    while running:
        still = []
        for steps in running:
            try:
                next(steps)
                still.append(steps)
            except StopIteration:
                pass
        running = still

    outgoing.append(bring(final_x, out_x))
    for copy in swaps + sent:
        copy.wait_send()
    for copy in outgoing:
        copy.wait()


def blocks(pieces, act, rank, column, gain_in, w_q, w_f, w_v, w_g, minimum, extra, gain_out, emission, memory):
    capacity = sum(rows for _, rows in pieces)
    anywhere = pl.BlockSpec(memory_space=pl.ANY)
    vmem = pl.BlockSpec(memory_space=pltpu.VMEM)
    scratch = [
        pltpu.VMEM((RING, SHARD_ROWS, 2 * FEATURES), BF16),
        pltpu.VMEM((BLOCKS, FEATURES), F32),
        pltpu.VMEM((BLOCKS, 2 * FEATURES, 4 * CHANNELS), BF16),
        pltpu.VMEM((BLOCKS, CHANNELS, 2 * FEATURES), BF16),
        pltpu.VMEM((BLOCKS, SEQS, HEADS, LANES, LANES), F32),
        pltpu.VMEM((RING * max(rows for _, rows in pieces), 2 * FEATURES), BF16),
        pltpu.VMEM((BLOCKS, 4 * HEADS, SHARD_ROWS, LANES), F32),
        pltpu.VMEM((HEADS, SHARD_ROWS, LANES), F32),
        pltpu.VMEM((HEADS, SHARD_ROWS, LANES), F32),
        pltpu.VMEM((SHARD_ROWS, CHANNELS), F32),
        pltpu.VMEM((BLOCKS, SHARD_ROWS, LANES), F32),
        pltpu.VMEM((BLOCKS, HEADS, SHARD_ROWS, LANES), F32),
        pltpu.VMEM((BLOCKS, SEQS, CHANNELS), F32),
        pltpu.VMEM((2, RING, capacity, FEATURES), BF16),
        pltpu.SemaphoreType.DMA((32,)),
        pltpu.SemaphoreType.DMA((16,)),
        pltpu.SemaphoreType.DMA((16,)),
        pltpu.SemaphoreType.DMA((BLOCKS, len(pieces), 9, RING)),
        pltpu.SemaphoreType.DMA((BLOCKS, len(pieces), 9, RING)),
    ]
    for _, rows in pieces:
        scratch += [
            pltpu.VMEM((BLOCKS, RING, rows, FEATURES), BF16),
            pltpu.VMEM((BLOCKS, RING, rows, FEATURES), BF16),
            pltpu.VMEM((BLOCKS, RING, rows, 4 * CHANNELS), BF16),
            pltpu.VMEM((BLOCKS, RING - 1, rows, 4 * CHANNELS), BF16),
            pltpu.VMEM((BLOCKS, RING, 1, LANES), F32),
            pltpu.VMEM((BLOCKS, RING - 1, 1, LANES), F32),
            pltpu.VMEM((BLOCKS, RING, rows, CHANNELS), BF16),
            pltpu.VMEM((BLOCKS, RING, rows, FEATURES), BF16),
            pltpu.VMEM((BLOCKS, RING, rows, FEATURES), BF16),
            pltpu.VMEM((BLOCKS, 2, RING - 1, rows, FEATURES), BF16),
            pltpu.VMEM((BLOCKS, RING, rows, FEATURES), BF16),
            pltpu.VMEM((BLOCKS, RING, rows, FEATURES), BF16),
            pltpu.VMEM((rows, FEATURES), BF16),
        ]
    return pl.pallas_call(
        functools.partial(blocks_kernel, pieces),
        out_shape=(
            jax.ShapeDtypeStruct((2, RING, capacity, FEATURES), BF16),
            jax.ShapeDtypeStruct((BLOCKS, HEADS, SHARD_ROWS, LANES), F32),
            jax.ShapeDtypeStruct((BLOCKS, HEADS, SHARD_ROWS, LANES), F32),
            jax.ShapeDtypeStruct((BLOCKS, SEQS, CHANNELS), F32),
        ),
        in_specs=[anywhere, vmem, vmem, vmem, anywhere, anywhere, anywhere, anywhere, vmem, vmem, vmem, anywhere, anywhere],
        out_specs=(anywhere,) * 4,
        scratch_shapes=scratch,
        compiler_params=pltpu.CompilerParams(
            collective_id=len(pieces) + capacity, has_side_effects=True, vmem_limit_bytes=VMEM_BYTES
        ),
        name="blocks",
    )(act, rank, column, gain_in, w_q, w_f, w_v, w_g, minimum, extra, gain_out, emission, memory)


GROUP = 8


def outputs_kernel(keys, values, decay, memory, rank, rows, act, mixed, states):
    g = pl.program_id(1)
    diagonal = iota((LANES, LANES), 0) == iota((LANES, LANES), 1)
    for unit in range(GROUP):
        s = g * GROUP + unit
        slots = pl.ds(s, SLOTS, stride=SEQS)
        for head in range(HEADS):
            low, high = head * LANES, (head + 1) * LANES
            added = dot_rows(keys[0, head, slots, :].astype(BF16), values[0, head, slots, :].astype(BF16))
            total = decay[0, unit : unit + 1, low:high]
            kept = jnp.sum(jnp.where(diagonal, total, 0.0), axis=1, keepdims=True)
            states[0, unit, head] = kept * memory[0, unit, head] + added
    capacity = rows.shape[2]
    places = chosen(rank[0], 0, capacity)
    live = dot_rows(places, jnp.ones((capacity, LANES), BF16)) > 0.5
    spread = dot_rows(places, rows[0, 0]).astype(BF16)
    for part in range(FEATURES // LANES):
        columns = slice(part * LANES, (part + 1) * LANES)
        mixed[:, columns] = jnp.where(live, spread[:, columns], act[:, columns])


def write_out(rows, keys, values, decay, memory, rank, act):
    capacity = rows.shape[2]
    steps = SEQS // GROUP

    def shard(b, g):
        return b * steps + g

    return pl.pallas_call(
        outputs_kernel,
        grid=(BLOCKS, steps),
        out_shape=(
            jax.ShapeDtypeStruct(act.shape, BF16),
            jax.ShapeDtypeStruct(memory.shape, F32),
        ),
        in_specs=[
            pl.BlockSpec((1, HEADS, SHARD_ROWS, LANES), lambda b, g: (b, 0, 0, 0)),
            pl.BlockSpec((1, HEADS, SHARD_ROWS, LANES), lambda b, g: (b, 0, 0, 0)),
            pl.BlockSpec((1, GROUP, CHANNELS), lambda b, g: (b, g, 0)),
            pl.BlockSpec((1, GROUP, HEADS, LANES, LANES), lambda b, g: (b, g, 0, 0, 0)),
            pl.BlockSpec((1, 1, SHARD_ROWS), lambda b, g: (shard(b, g), 0, 0)),
            pl.BlockSpec(
                (1, 1, capacity, FEATURES), lambda b, g: (lax.rem(shard(b, g), 2), lax.div(shard(b, g), 2), 0, 0)
            ),
            pl.BlockSpec((SHARD_ROWS, FEATURES), lambda b, g: (b * steps + g, 0)),
        ],
        out_specs=(
            pl.BlockSpec((SHARD_ROWS, FEATURES), lambda b, g: (b * steps + g, 0)),
            pl.BlockSpec((1, GROUP, HEADS, LANES, LANES), lambda b, g: (b, g, 0, 0, 0)),
        ),
        name="write_out",
    )(keys, values, decay, memory, rank, rows, act)


FEW = ((0, 64), (64, 64))
ALL = ((0, 128), (128, 128))


def local(
    activation_rows,
    fresh_spans,
    entry_rescale_vector,
    probe_kernel,
    retention_kernel,
    content_kernel,
    valve_kernel,
    retention_minimum,
    extra_attenuation,
    channel_rescale_vector,
    emission_kernel,
    memory_grids,
):
    rank, column = tables(fresh_spans.reshape(1, SEQS))

    def run(pieces, *args):
        act, memory = args[0], args[-1]
        rows, keys, values, decay = blocks(pieces, *args)
        return write_out(rows, keys, values, decay, memory, args[1], act)

    capacity = sum(rows for _, rows in FEW)
    return lax.cond(
        jnp.max(rank) < capacity,
        functools.partial(run, FEW),
        functools.partial(run, ALL),
        activation_rows,
        rank,
        column,
        entry_rescale_vector,
        probe_kernel,
        retention_kernel,
        content_kernel,
        valve_kernel,
        retention_minimum,
        extra_attenuation,
        channel_rescale_vector,
        emission_kernel,
        memory_grids,
    )


def solution(mesh):
    placed = (
        P(None, "dp"),
        P("dp"),
        P(None, "dp"),
        P(None, "dp", "tp"),
        P(None, "dp", "tp"),
        P(None, "dp", "tp"),
        P(None, "dp", "tp"),
        P(None, "tp"),
        P(None, "dp", "tp"),
        P(None, "tp"),
        P(None, "tp", "dp"),
        P(None, "dp", "tp", None, None),
    )
    return jax.shard_map(
        local,
        mesh=mesh,
        in_specs=placed,
        out_specs=(P(None, "dp"), P(None, "dp", "tp", None, None)),
        check_vma=False,
    )
```

```python
import functools

import jax
import jax.numpy as jnp
from jax import lax
from jax.experimental import pallas as pl
from jax.experimental.pallas import tpu as pltpu
from jax.sharding import PartitionSpec as P

D = 4096
BLOCKS = 2
EPSILON = 1e-05
RING = 4
SHARDS = 8
SEQS = 32
SLOTS = 8
SHARD_ROWS = SEQS * SLOTS
FEATURES = 512
CHANNELS = 256
HEADS = 2
LANES = 128
MESH = pl.DeviceIdType.MESH
F32 = jnp.float32
BF16 = jnp.bfloat16
VMEM_BYTES = 44 * 1024 * 1024


def here():
    dp, tp = lax.axis_index("dp"), lax.axis_index("tp")
    return lax.div(dp, 2), lax.rem(dp, 2), lax.div(tp, RING), lax.rem(tp, RING)


def device(x, core, z, y):
    return {"tp": z * RING + y, "dp": x * 2 + core}


def around(index, offset):
    return lax.rem(index + offset, RING)


def greet(peers):
    barrier = pltpu.get_barrier_semaphore()
    for peer in peers:
        pl.semaphore_signal(barrier, inc=1, device_id=peer, device_id_type=MESH)
    pl.semaphore_wait(barrier, len(peers))


def iota(shape, dim):
    return lax.broadcasted_iota(jnp.int32, shape, dim)


def dot(a, b):
    return jnp.dot(a, b, preferred_element_type=F32)


def dot_rows(a, b):
    return lax.dot_general(a, b, (((0,), (0,)), ((), ())), preferred_element_type=F32)


def chosen(rank_row, first, count):
    wanted = (iota((count, rank_row.shape[1]), 0) + first).astype(F32)
    return jnp.where(wanted == rank_row, 1.0, 0.0).astype(BF16)


def tables_kernel(
    spans, act, gain_in, w_q, w_f, w_v, w_g,
    rank, column, many, raw, gain_peer, weights,
    gathered, send_sems, recv_sems, local_sems, swap_send, swap_recv,
):
    x, core, z, y = here()
    dp, tp = x * 2 + core, z * RING + y
    others = [{"tp": tp, "dp": lax.rem(dp + offset, SHARDS)} for offset in range(1, SHARDS)]
    partner = device(x, 1 - core, z, y)
    kernels = (w_q, w_f, w_v, w_g)

    def rows_of(side, j):
        return act.at[pl.ds((j * 2 + side) * SHARD_ROWS, SHARD_ROWS), :]

    moves = [(rows_of(core, j), raw.at[j, :, 0:FEATURES]) for j in range(RING)]
    moves += [(kernels[k].at[0], weights.at[0:FEATURES, k * CHANNELS : (k + 1) * CHANNELS]) for k in range(4)]
    local = []
    for number, (source, target) in enumerate(moves):
        copy = pltpu.make_async_copy(source, target, local_sems.at[number])
        copy.start()
        local.append(copy)

    greet(others)
    copies = []
    for number, other in enumerate(others):
        copy = pltpu.make_async_remote_copy(
            spans,
            gathered.at[dp],
            send_sems.at[number],
            recv_sems.at[number],
            device_id=other,
            device_id_type=MESH,
        )
        copy.start()
        copies.append(copy)
    moves = [(rows_of(1 - core, j), raw.at[j, :, FEATURES : 2 * FEATURES]) for j in range(RING)]
    moves += [
        (kernels[k].at[0], weights.at[FEATURES : 2 * FEATURES, k * CHANNELS : (k + 1) * CHANNELS]) for k in range(4)
    ]
    moves += [(gain_in, gain_peer)]
    swaps = []
    for number, (source, target) in enumerate(moves):
        copy = pltpu.make_async_remote_copy(
            source,
            target,
            swap_send.at[number],
            swap_recv.at[number],
            device_id=partner,
            device_id_type=MESH,
        )
        copy.start()
        swaps.append(copy)
    gathered[dp] = spans[...]

    own = spans[...].astype(F32)
    lane, row = iota((SEQS, SEQS), 1), iota((SEQS, SEQS), 0)
    before = jnp.sum(jnp.where(lane < row, own, 0.0), axis=1, keepdims=True)
    same = jnp.sum(jnp.where(lane == row, own, 0.0), axis=1, keepdims=True)
    column[0:SEQS, :] = jnp.broadcast_to(before, (SEQS, LANES))
    column[SEQS:, :] = jnp.broadcast_to(same, (SEQS, LANES))

    for copy in copies:
        copy.wait_recv()
    spans_all = jnp.concatenate([gathered[index] for index in range(SHARDS)], axis=0).astype(F32)
    most = jnp.max(jnp.sum(spans_all, axis=1, keepdims=True))
    many[0, 0] = jnp.where(most > CAPACITY, 1, 0)
    spans_all = spans_all.astype(BF16)
    slot_index = iota((SEQS, SHARD_ROWS), 1)
    sequence = iota((SEQS, SHARD_ROWS), 0)
    for order in range(2):
        if order == 0:
            owner, position = lax.shift_right_logical(slot_index, 3), slot_index & 7
        else:
            owner, position = slot_index & 31, lax.shift_right_logical(slot_index, 5)
        earlier = jnp.where(sequence < owner, 1.0, 0.0).astype(BF16)
        equal = jnp.where(sequence == owner, 1.0, 0.0).astype(BF16)
        start, length = dot(spans_all, earlier), dot(spans_all, equal)
        place = position[0:SHARDS].astype(F32)
        ranks = jnp.where(place < length, start + place, -1.0)
        for index in range(SHARDS):
            rank[order * SHARDS + index] = ranks[index : index + 1]
    for copy in local:
        copy.wait()
    for copy in swaps:
        copy.wait()
    for copy in copies:
        copy.wait_send()


def tables(spans, act, gain_in, *kernels):
    anywhere = pl.BlockSpec(memory_space=pl.ANY)
    vmem = pl.BlockSpec(memory_space=pltpu.VMEM)
    return pl.pallas_call(
        tables_kernel,
        out_shape=(
            jax.ShapeDtypeStruct((2 * SHARDS, 1, SHARD_ROWS), F32),
            jax.ShapeDtypeStruct((2 * SEQS, LANES), F32),
            jax.ShapeDtypeStruct((1, 1), jnp.int32),
            jax.ShapeDtypeStruct((RING, SHARD_ROWS, 2 * FEATURES), BF16),
            jax.ShapeDtypeStruct((BLOCKS, FEATURES), F32),
            jax.ShapeDtypeStruct((2 * FEATURES, 4 * CHANNELS), BF16),
        ),
        in_specs=[vmem, anywhere, vmem] + [anywhere] * 4,
        out_specs=(vmem, vmem, pl.BlockSpec(memory_space=pltpu.SMEM), vmem, vmem, vmem),
        scratch_shapes=[
            pltpu.VMEM((SHARDS, 1, SEQS), jnp.int32),
            pltpu.SemaphoreType.DMA((SHARDS - 1,)),
            pltpu.SemaphoreType.DMA((SHARDS - 1,)),
            pltpu.SemaphoreType.DMA((8,)),
            pltpu.SemaphoreType.DMA((9,)),
            pltpu.SemaphoreType.DMA((9,)),
        ],
        compiler_params=pltpu.CompilerParams(
            collective_id=0, has_side_effects=True, vmem_limit_bytes=8 * 1024 * 1024
        ),
        name="live_tables",
    )(spans, act, gain_in, *kernels)


def silu(a):
    return a * jax.nn.sigmoid(a)


def gates(b, hi, refs):
    spread, column, minimum, added, q_decayed, own_read, keys, decay_total = refs
    ones = jnp.ones((LANES, LANES), BF16)

    def group(g, carry):
        start = column[pl.ds(pl.multiple_of(g * 8, 8), 8), :]
        span = column[pl.ds(pl.multiple_of(SEQS + g * 8, 8), 8), :]
        for head in range(HEADS):
            low, high = head * LANES, (head + 1) * LANES
            floor = minimum[b : b + 1, low:high]
            kept, values, products = [], [], []
            running = None
            for p in range(SLOTS):
                rows = pl.ds(pl.multiple_of(p * SEQS + g * 8, 8), 8)
                q = silu(spread[b, head, rows, :])
                f = spread[b, HEADS + head, rows, :]
                values.append(spread[b, 2 * HEADS + head, rows, :])
                small = jnp.exp(-jnp.abs(f))
                large = 1.0 / (1.0 + small)
                small = small * large
                up = f >= 0.0
                live = jnp.logical_and(span > p, start + p < hi)
                forget = floor + (1.0 - floor) * jnp.where(up, large, small)
                decay = jnp.where(live, forget * added[b, head, pl.ds(g * 64 + p, 8, stride=8), :], 1.0)
                key = jnp.where(live, (1.0 - floor) * jnp.where(up, small, large), 0.0)
                running = decay if p == 0 else running * decay
                kept = [old * decay for old in kept] + [key]
                products += [q * old for old in kept]
                q_decayed[head, rows, :] = q * running
            for p in range(SLOTS):
                rows = pl.ds(pl.multiple_of(p * SEQS + g * 8, 8), 8)
                keys[b, head, rows, :] = kept[p]
            decay_total[b, pl.ds(pl.multiple_of(g * 8, 8), 8), low:high] = running
            scores = dot(jnp.concatenate(products, axis=0).astype(BF16), ones)
            number = 0
            for p in range(SLOTS):
                read = None
                for value in values[: p + 1]:
                    term = scores[number * 8 : (number + 1) * 8] * value
                    read = term if read is None else read + term
                    number += 1
                own_read[head, pl.ds(pl.multiple_of(p * SEQS + g * 8, 8), 8), :] = read
        return carry

    lax.fori_loop(0, SEQS // 8, group, 0)


def reads(b, refs):
    spread, rounded, gain, q_decayed, own_read, heads_out = refs
    together = 4

    def group(g, carry):
        for unit in range(together):
            s = g * together + unit
            rows = pl.ds(s, SLOTS, stride=SEQS)
            for head in range(HEADS):
                low, high = head * LANES, (head + 1) * LANES
                read = dot(q_decayed[head, rows, :].astype(BF16), rounded[s, head])
                read = read + own_read[head, rows, :]
                square = jnp.mean(read * read, axis=1, keepdims=True)
                gate = silu(spread[b, 3 * HEADS + head, rows, :])
                out = read * lax.rsqrt(square + EPSILON) * gain[b : b + 1, low:high] * gate
                heads_out[pl.ds(pl.multiple_of(s * SLOTS, SLOTS), SLOTS), low:high] = out
        return carry

    lax.fori_loop(0, SEQS // together, group, 0)


def round_states(b, states, rounded):
    def group(g, carry):
        rounded[pl.ds(g * 4, 4)] = states[b, pl.ds(g * 4, 4)].astype(BF16)
        return carry

    lax.fori_loop(0, SEQS // 4, group, 0)


def advance_states(b, first, number, refs):
    states, spread, keys, decay_total = refs

    def group(g, carry):
        diagonal = iota((LANES, LANES), 0) == iota((LANES, LANES), 1)
        totals = decay_total[b, pl.ds(pl.multiple_of(g * 8, 8), 8), :]
        for unit in range(8):
            s = g * 8 + unit
            slots = pl.ds(s, SLOTS, stride=SEQS)
            for head in range(HEADS):
                added = dot_rows(
                    keys[b, head, slots, :].astype(BF16), spread[b, 2 * HEADS + head, slots, :].astype(BF16)
                )
                total = totals[unit : unit + 1, head * LANES : (head + 1) * LANES]
                kept = jnp.sum(jnp.where(diagonal, total, 0.0), axis=1, keepdims=True)
                states[b, s, head] = kept * states[b, s, head] + added
        return carry

    lax.fori_loop(first, first + number, group, 0)


def blocks_kernel(pieces, *refs):
    count = len(pieces)
    (rank, column, raw, gain_peer, first_weights, gain_in, w_q, w_f, w_v, w_g) = refs[:10]
    (minimum, extra, gain_out, emission, memory, final_x, states) = refs[10:17]
    refs = list(refs[17:])

    def take(number):
        taken = refs[:number]
        del refs[:number]
        return taken

    (later_weights, outward, rounded, normed, spread, q_decayed, own_read, heads_out, added, keys, decay_total) = take(11)
    (local_sems, swap_send, swap_recv, send_sems, recv_sems) = take(5)
    per = [take(13) for _ in range(count)]
    x, core, z, y = here()
    dp = x * 2 + core

    xs = [device(around(x, o), core, z, y) for o in range(1, RING)]
    ys = [device(x, core, z, around(y, o)) for o in range(1, RING)]
    zs = [device(x, core, around(z, o), y) for o in range(1, RING)]
    crossed = [device(x, 1 - core, around(z, o), y) for o in range(RING)]
    partner = crossed[0]
    kernels = (w_q, w_f, w_v, w_g)

    local, swaps, sent = [], [], []

    def bring(source, target):
        copy = pltpu.make_async_copy(source, target, local_sems.at[len(local)])
        copy.start()
        local.append(copy)
        return copy

    def swap(source, target):
        number = len(swaps)
        copy = pltpu.make_async_remote_copy(
            source,
            target,
            swap_send.at[number],
            swap_recv.at[number],
            device_id=partner,
            device_id_type=MESH,
        )
        copy.start()
        swaps.append(copy)
        return copy

    def send(b, i, phase, number, source, target, peer):
        copy = pltpu.make_async_remote_copy(
            source,
            target,
            send_sems.at[b, i, phase, number],
            recv_sems.at[b, i, phase, number],
            device_id=peer,
            device_id_type=MESH,
        )
        copy.start()
        sent.append(copy)
        return copy

    own_states = [bring(memory.at[b], states.at[b]) for b in range(BLOCKS)]
    own_outward = [bring(emission.at[b], outward.at[b, :, 0:FEATURES]) for b in range(BLOCKS)]
    own_weights = [
        bring(kernels[k].at[1], later_weights.at[0:FEATURES, k * CHANNELS : (k + 1) * CHANNELS]) for k in range(4)
    ]

    greet(xs + ys + zs + crossed)

    peer_outward = [swap(emission.at[b], outward.at[b, :, FEATURES : 2 * FEATURES]) for b in range(BLOCKS)]
    peer_weights = [
        swap(kernels[k].at[1], later_weights.at[FEATURES : 2 * FEATURES, k * CHANNELS : (k + 1) * CHANNELS])
        for k in range(4)
    ]
    waiting = []

    def piece_steps(i):
        first, rows = pieces[i]
        (x_own, x_peer, parts, got, squares, got_squares, heads, u_own, u_peer, one, two_own, two_peer, last_peer) = per[i]
        for j in range(RING):
            picked = dot(chosen(rank[j * 2 + core], first, rows), raw[j]).astype(BF16)
            x_own[0, j] = picked[:, 0:FEATURES]
            x_peer[0, j] = picked[:, FEATURES:]
        for b in range(BLOCKS):
            weights = later_weights if b else first_weights
            eye = iota((rows, LANES), 0) == iota((rows, LANES), 1)
            for j in range(RING):
                a = x_own[b, j].astype(F32)
                c = x_peer[b, j].astype(F32)
                total = jnp.sum(a * a, axis=1, keepdims=True) + jnp.sum(c * c, axis=1, keepdims=True)
                squares[b, j] = jnp.sum(jnp.where(eye, total, 0.0), axis=0, keepdims=True)
                normed[j * rows : (j + 1) * rows, 0:FEATURES] = (a * gain_in[b : b + 1]).astype(BF16)
                normed[j * rows : (j + 1) * rows, FEATURES:] = (c * gain_peer[b : b + 1]).astype(BF16)
            waits = []
            for o in (2, 1, 3):
                waits.append(
                    send(b, i, 1, o - 1, squares.at[b, around(x, o)], got_squares.at[b, o - 1], xs[o - 1])
                )
            if i == 0 and b == 1:
                for k in range(4):
                    own_weights[k].wait()
                    peer_weights[k].wait_recv()

            def project(k, carry, b=b, weights=weights):
                columns = pl.ds(pl.multiple_of(k * CHANNELS, CHANNELS), CHANNELS)
                product = dot(normed[0 : RING * rows], weights[:, columns]).astype(BF16)
                for j in range(RING):
                    parts[b, j, :, columns] = product[j * rows : (j + 1) * rows]
                return carry

            lax.fori_loop(0, 4, project, 0)
            for o in (2, 1, 3):
                waits.append(send(b, i, 0, o - 1, parts.at[b, around(x, o)], got.at[b, o - 1], xs[o - 1]))
            if i == count - 1:
                if b == 0:
                    widen()
                own_states[b].wait()
                round_states(b, states, rounded)
            yield

            for wait in waits:
                wait.wait_recv()
            square = squares[b, x] + got_squares[b, 0] + got_squares[b, 1] + got_squares[b, 2]
            scale_row = lax.rsqrt(square / D + EPSILON)
            scale = jnp.sum(jnp.where(eye, scale_row, 0.0), axis=1, keepdims=True)
            places = chosen(rank[SHARDS + dp], first, rows)

            def expand(k, carry, b=b, scale=scale, places=places):
                columns = pl.ds(pl.multiple_of(k * CHANNELS, CHANNELS), CHANNELS)
                total = parts[b, x, :, columns].astype(F32)
                for o in range(RING - 1):
                    total = total + got[b, o, :, columns].astype(F32)
                placed = dot_rows(places, (total * scale).astype(BF16))
                for head in range(HEADS):
                    part = placed[:, head * LANES : (head + 1) * LANES]
                    if i > 0:
                        part = part + spread[b, k * HEADS + head]
                    spread[b, k * HEADS + head] = part
                return carry

            lax.fori_loop(0, 4, expand, 0)
            gates(b, first + rows, (spread, column, minimum, added, q_decayed, own_read, keys, decay_total))
            reads(b, (spread, rounded, gain_out, q_decayed, own_read, heads_out))
            heads[b, x] = dot(chosen(rank[dp], first, rows), heads_out[...].astype(BF16)).astype(BF16)
            waits = [send(b, i, 2, o - 1, heads.at[b, x], heads.at[b, x], xs[o - 1]) for o in (2, 1, 3)]
            if i == count - 1:
                for g in range(SEQS // 8):
                    waiting.append(
                        functools.partial(advance_states, b, g, 1, (states, spread, keys, decay_total))
                    )
            if i == 0:
                own_outward[b].wait()
                peer_outward[b].wait_recv()
            yield

            for wait in waits:
                wait.wait_recv()
            all_heads = heads[b].reshape(RING * rows, CHANNELS)
            for half, target in enumerate((u_own, u_peer)):
                for part in range(2):
                    low = part * CHANNELS
                    columns = slice(half * FEATURES + low, half * FEATURES + low + CHANNELS)
                    product = dot(all_heads, outward[b, :, columns]).astype(BF16)
                    for j in range(RING):
                        target[b, j, :, low : low + CHANNELS] = product[j * rows : (j + 1) * rows]
            waits = []
            for o in (2, 1, 3):
                waits.append(send(b, i, 3, o - 1, u_own.at[b, around(y, o)], one.at[b, 0, o - 1], ys[o - 1]))
                waits.append(send(b, i, 4, o - 1, u_peer.at[b, around(z, o)], one.at[b, 1, o - 1], zs[o - 1]))
            yield

            for wait in waits:
                wait.wait_recv()
            waits = []
            for half, (mine, at, slots, own, peers) in enumerate(
                ((u_own, y, two_own, z, zs), (u_peer, z, two_peer, y, ys))
            ):
                total = mine[b, at].astype(F32)
                for o in range(RING - 1):
                    total = total + one[b, half, o].astype(F32)
                slots[b, own] = total.astype(BF16)
                for o in (2, 1, 3):
                    waits.append(send(b, i, 5 + half, o - 1, slots.at[b, own], slots.at[b, own], peers[o - 1]))
            yield

            for wait in waits:
                wait.wait_recv()
            waits = []
            for half, (slots, old, at) in enumerate(((two_own, x_own, y), (two_peer, x_peer, z))):
                total = slots[b, 0].astype(F32)
                for o in range(1, RING):
                    total = total + slots[b, o].astype(F32)
                fresh = (old[b, at].astype(F32) + total.astype(BF16).astype(F32)).astype(BF16)
                if b < BLOCKS - 1:
                    old[b + 1, at] = fresh
                    peers = ys if half == 0 else zs
                    for o in (2, 1, 3):
                        waits.append(send(b, i, 7 + half, o - 1, old.at[b + 1, at], old.at[b + 1, at], peers[o - 1]))
                elif half == 0:
                    place = final_x.at[core, y, first : first + rows]
                    final_x[core, y, first : first + rows] = fresh
                    for o in (2, 1, 3):
                        waits.append(send(b, i, 7, o - 1, place, place, ys[o - 1]))
                else:
                    last_peer[...] = fresh
                    place = final_x.at[core, z, first : first + rows]
                    for o in (2, 1, 3, 0):
                        waits.append(send(b, i, 8, o, last_peer, place, crossed[o]))
            yield
            for wait in waits:
                wait.wait_recv()

    def widen():
        diagonal = iota((LANES, LANES), 0) == iota((LANES, LANES), 1)
        for b in range(BLOCKS):
            for head in range(HEADS):
                for part in range(SHARD_ROWS // LANES):
                    row = extra[b, head : head + 1, part * LANES : (part + 1) * LANES]
                    wide = jnp.sum(jnp.where(diagonal, jnp.exp(row), 0.0), axis=1, keepdims=True)
                    added[b, head, part * LANES : (part + 1) * LANES, :] = jnp.broadcast_to(wide, (LANES, LANES))

    running = [piece_steps(i) for i in range(count)]
    while running:
        still = []
        for steps in running:
            try:
                next(steps)
                still.append(steps)
            except StopIteration:
                pass
            if waiting:
                waiting.pop(0)()
        running = still

    for work in waiting:
        work()
    for copy in swaps + sent:
        copy.wait_send()


def blocks(pieces, *args):
    capacity = sum(rows for _, rows in pieces)
    anywhere = pl.BlockSpec(memory_space=pl.ANY)
    vmem = pl.BlockSpec(memory_space=pltpu.VMEM)
    scratch = [
        pltpu.VMEM((2 * FEATURES, 4 * CHANNELS), BF16),
        pltpu.VMEM((BLOCKS, CHANNELS, 2 * FEATURES), BF16),
        pltpu.VMEM((SEQS, HEADS, LANES, LANES), BF16),
        pltpu.VMEM((RING * max(rows for _, rows in pieces), 2 * FEATURES), BF16),
        pltpu.VMEM((BLOCKS, 4 * HEADS, SHARD_ROWS, LANES), F32),
        pltpu.VMEM((HEADS, SHARD_ROWS, LANES), F32),
        pltpu.VMEM((HEADS, SHARD_ROWS, LANES), F32),
        pltpu.VMEM((SHARD_ROWS, CHANNELS), F32),
        pltpu.VMEM((BLOCKS, HEADS, SHARD_ROWS, LANES), F32),
        pltpu.VMEM((BLOCKS, HEADS, SHARD_ROWS, LANES), F32),
        pltpu.VMEM((BLOCKS, SEQS, CHANNELS), F32),
        pltpu.SemaphoreType.DMA((8,)),
        pltpu.SemaphoreType.DMA((6,)),
        pltpu.SemaphoreType.DMA((6,)),
        pltpu.SemaphoreType.DMA((BLOCKS, len(pieces), 9, RING)),
        pltpu.SemaphoreType.DMA((BLOCKS, len(pieces), 9, RING)),
    ]
    for _, rows in pieces:
        scratch += [
            pltpu.VMEM((BLOCKS, RING, rows, FEATURES), BF16),
            pltpu.VMEM((BLOCKS, RING, rows, FEATURES), BF16),
            pltpu.VMEM((BLOCKS, RING, rows, 4 * CHANNELS), BF16),
            pltpu.VMEM((BLOCKS, RING - 1, rows, 4 * CHANNELS), BF16),
            pltpu.VMEM((BLOCKS, RING, 1, LANES), F32),
            pltpu.VMEM((BLOCKS, RING - 1, 1, LANES), F32),
            pltpu.VMEM((BLOCKS, RING, rows, CHANNELS), BF16),
            pltpu.VMEM((BLOCKS, RING, rows, FEATURES), BF16),
            pltpu.VMEM((BLOCKS, RING, rows, FEATURES), BF16),
            pltpu.VMEM((BLOCKS, 2, RING - 1, rows, FEATURES), BF16),
            pltpu.VMEM((BLOCKS, RING, rows, FEATURES), BF16),
            pltpu.VMEM((BLOCKS, RING, rows, FEATURES), BF16),
            pltpu.VMEM((rows, FEATURES), BF16),
        ]
    return pl.pallas_call(
        functools.partial(blocks_kernel, pieces),
        out_shape=(
            jax.ShapeDtypeStruct((2, RING, capacity, FEATURES), BF16),
            jax.ShapeDtypeStruct((BLOCKS, SEQS, HEADS, LANES, LANES), F32),
        ),
        in_specs=[vmem] * 6 + [anywhere] * 4 + [vmem] * 3 + [anywhere] * 2,
        out_specs=(vmem, vmem),
        scratch_shapes=scratch,
        compiler_params=pltpu.CompilerParams(
            collective_id=len(pieces) + capacity, has_side_effects=True, vmem_limit_bytes=VMEM_BYTES
        ),
        name="blocks",
    )(*args)


def outputs_kernel(rank, rows, held, act, mixed, states, old, fresh, state_sems, in_sems, out_sems):
    capacity = rows.shape[2]
    shard_rows = [pl.ds(d * SHARD_ROWS, SHARD_ROWS) for d in range(SHARDS)]
    loads = [pltpu.make_async_copy(act.at[shard_rows[d]], old.at[d], in_sems.at[d]) for d in range(SHARDS)]
    for load in loads:
        load.start()
    writes = [pltpu.make_async_copy(held.at[b], states.at[b], state_sems.at[b]) for b in range(BLOCKS)]
    for write in writes:
        write.start()
    for load in loads:
        load.wait()

    def shard(d, carry):
        places = chosen(rank[d], 0, capacity)
        live = dot_rows(places, jnp.ones((capacity, LANES), BF16)) > 0.5
        spread = dot_rows(places, rows[lax.rem(d, 2), lax.div(d, 2)]).astype(BF16)
        for part in range(FEATURES // LANES):
            columns = slice(part * LANES, (part + 1) * LANES)
            fresh[d, :, columns] = jnp.where(live, spread[:, columns], old[d, :, columns])
        return carry

    lax.fori_loop(0, SHARDS, shard, 0)
    for d in range(SHARDS):
        write = pltpu.make_async_copy(fresh.at[d], mixed.at[shard_rows[d]], out_sems.at[d])
        write.start()
        writes.append(write)
    for write in writes:
        write.wait()


def write_out(rank, rows, held, act):
    anywhere = pl.BlockSpec(memory_space=pl.ANY)
    vmem = pl.BlockSpec(memory_space=pltpu.VMEM)
    return pl.pallas_call(
        outputs_kernel,
        out_shape=(
            jax.ShapeDtypeStruct(act.shape, BF16),
            jax.ShapeDtypeStruct(held.shape, F32),
        ),
        in_specs=[vmem, vmem, vmem, anywhere],
        out_specs=(anywhere, anywhere),
        scratch_shapes=[
            pltpu.VMEM((SHARDS, SHARD_ROWS, FEATURES), BF16),
            pltpu.VMEM((SHARDS, SHARD_ROWS, FEATURES), BF16),
            pltpu.SemaphoreType.DMA((BLOCKS,)),
            pltpu.SemaphoreType.DMA((SHARDS,)),
            pltpu.SemaphoreType.DMA((SHARDS,)),
        ],
        compiler_params=pltpu.CompilerParams(vmem_limit_bytes=16 * 1024 * 1024),
        name="write_out",
    )(rank, rows, held, act)


CAPACITY = 128
FEW = ((0, 64), (64, 64))
ALL = ((0, 128), (128, 128))


def local(
    activation_rows,
    fresh_spans,
    entry_rescale_vector,
    probe_kernel,
    retention_kernel,
    content_kernel,
    valve_kernel,
    retention_minimum,
    extra_attenuation,
    channel_rescale_vector,
    emission_kernel,
    memory_grids,
):
    kernels = (probe_kernel, retention_kernel, content_kernel, valve_kernel)
    rank, column, many, raw, gain_peer, first_weights = tables(
        fresh_spans.reshape(1, SEQS), activation_rows, entry_rescale_vector, *kernels
    )

    def run(pieces, act, *args):
        rows, held = blocks(pieces, *args)
        return write_out(args[0], rows, held, act)

    return lax.cond(
        many[0, 0] == 0,
        functools.partial(run, FEW),
        functools.partial(run, ALL),
        activation_rows,
        rank,
        column,
        raw,
        gain_peer,
        first_weights,
        entry_rescale_vector,
        *kernels,
        retention_minimum,
        jnp.transpose(extra_attenuation, (0, 2, 1)),
        channel_rescale_vector,
        emission_kernel,
        memory_grids,
    )


def solution(mesh):
    placed = (
        P(None, "dp"),
        P("dp"),
        P(None, "dp"),
        P(None, "dp", "tp"),
        P(None, "dp", "tp"),
        P(None, "dp", "tp"),
        P(None, "dp", "tp"),
        P(None, "tp"),
        P(None, "dp", "tp"),
        P(None, "tp"),
        P(None, "tp", "dp"),
        P(None, "dp", "tp", None, None),
    )
    return jax.shard_map(
        local,
        mesh=mesh,
        in_specs=placed,
        out_specs=(P(None, "dp"), P(None, "dp", "tp", None, None)),
        check_vma=False,
    )
```

```python
import functools

import jax
import jax.numpy as jnp
from jax import lax
from jax.experimental import pallas as pl
from jax.experimental.pallas import tpu as pltpu
from jax.sharding import PartitionSpec as P

D = 4096
BLOCKS = 2
EPSILON = 1e-05
RING = 4
SHARDS = 8
SEQS = 32
SLOTS = 8
SHARD_ROWS = SEQS * SLOTS
FEATURES = 512
CHANNELS = 256
HEADS = 2
LANES = 128
MESH = pl.DeviceIdType.MESH
F32 = jnp.float32
BF16 = jnp.bfloat16
CHUNKS = 2
ADVANCES = {(2, False): 3, (2, True): 1, (3, False): 1, (3, True): 1, (4, False): 1, (4, True): 1}
WIDE = FEATURES // CHUNKS
MIB = 1024 * 1024


def here():
    dp, tp = lax.axis_index("dp"), lax.axis_index("tp")
    return lax.div(dp, 2), lax.rem(dp, 2), lax.div(tp, RING), lax.rem(tp, RING)


def device(x, core, z, y):
    return {"tp": z * RING + y, "dp": x * 2 + core}


def around(index, offset):
    return lax.rem(index + offset, RING)


def greet(peers):
    barrier = pltpu.get_barrier_semaphore()
    for peer in peers:
        pl.semaphore_signal(barrier, inc=1, device_id=peer, device_id_type=MESH)
    pl.semaphore_wait(barrier, len(peers))


def iota(shape, dim):
    return lax.broadcasted_iota(jnp.int32, shape, dim)


def dot(a, b):
    return jnp.dot(a, b, preferred_element_type=F32)


def dot_rows(a, b):
    return lax.dot_general(a, b, (((0,), (0,)), ((), ())), preferred_element_type=F32)


def chosen(rank_row, first, count):
    wanted = (iota((count, rank_row.shape[1]), 0) + first).astype(F32)
    return jnp.where(wanted == rank_row, 1.0, 0.0).astype(BF16)


def fill_columns(spans, column):
    own = spans[...].astype(F32)
    lane, row = iota((SEQS, SEQS), 1), iota((SEQS, SEQS), 0)
    before = jnp.sum(jnp.where(lane < row, own, 0.0), axis=1, keepdims=True)
    same = jnp.sum(jnp.where(lane == row, own, 0.0), axis=1, keepdims=True)
    column[0:SEQS, :] = jnp.broadcast_to(before, (SEQS, LANES))
    column[SEQS:, :] = jnp.broadcast_to(same, (SEQS, LANES))


def fill_ranks(gathered, rank, many):
    spans_all = jnp.concatenate([gathered[index] for index in range(SHARDS)], axis=0).astype(F32)
    most = jnp.max(jnp.sum(spans_all, axis=1, keepdims=True))
    many[0, 0] = jnp.where(most > CAPACITY, 1, 0)
    spans_all = spans_all.astype(BF16)
    slot_index = iota((SEQS, SHARD_ROWS), 1)
    sequence = iota((SEQS, SHARD_ROWS), 0)
    for order in range(2):
        if order == 0:
            owner, position = lax.shift_right_logical(slot_index, 3), slot_index & 7
        else:
            owner, position = slot_index & 31, lax.shift_right_logical(slot_index, 5)
        earlier = jnp.where(sequence < owner, 1.0, 0.0).astype(BF16)
        equal = jnp.where(sequence == owner, 1.0, 0.0).astype(BF16)
        start, length = dot(spans_all, earlier), dot(spans_all, equal)
        place = position[0:SHARDS].astype(F32)
        ranks = jnp.where(place < length, start + place, -1.0)
        for index in range(SHARDS):
            rank[order * SHARDS + index] = ranks[index : index + 1]


def silu(a):
    return a * jax.nn.sigmoid(a)


def gates(b, head, lo, hi, refs):
    spread, column, minimum, added, q_decayed, own_read, keys, decay_total = refs
    ones = jnp.ones((LANES, LANES), BF16)
    low, high = head * LANES, (head + 1) * LANES
    done = lo // SLOTS // 8
    together = 2 if (SEQS // 8 - done) % 2 == 0 else 3

    def group(pair, carry):
        for unit in range(together):
            g = done + pair * together + unit
            start = column[pl.ds(pl.multiple_of(g * 8, 8), 8), :]
            span = column[pl.ds(pl.multiple_of(SEQS + g * 8, 8), 8), :]
            floor = minimum[b : b + 1, low:high]
            kept, values, products = [], [], []
            running = None
            for p in range(SLOTS):
                rows = pl.ds(pl.multiple_of(p * SEQS + g * 8, 8), 8)
                q = silu(spread[b, head, 0, rows, :])
                f = spread[b, head, 1, rows, :]
                values.append(spread[b, head, 2, rows, :])
                small = jnp.exp(-jnp.abs(f))
                large = 1.0 / (1.0 + small)
                small = small * large
                up = f >= 0.0
                live = jnp.logical_and(span > p, start + p < hi)
                forget = floor + (1.0 - floor) * jnp.where(up, large, small)
                decay = jnp.where(live, forget * added[b, head, pl.ds(g * 64 + p, 8, stride=8), :], 1.0)
                key = jnp.where(live, (1.0 - floor) * jnp.where(up, small, large), 0.0)
                running = decay if p == 0 else running * decay
                kept = [old * decay for old in kept] + [key]
                products += [q * old for old in kept]
                q_decayed[head, rows, :] = q * running
            for p in range(SLOTS):
                rows = pl.ds(pl.multiple_of(p * SEQS + g * 8, 8), 8)
                keys[b, head, rows, :] = kept[p]
            decay_total[b, pl.ds(pl.multiple_of(g * 8, 8), 8), low:high] = running
            scores = dot(jnp.concatenate(products, axis=0).astype(BF16), ones)
            number = 0
            for p in range(SLOTS):
                read = None
                for value in values[: p + 1]:
                    term = scores[number * 8 : (number + 1) * 8] * value
                    read = term if read is None else read + term
                    number += 1
                own_read[head, pl.ds(pl.multiple_of(p * SEQS + g * 8, 8), 8), :] = read
        return carry

    lax.fori_loop(0, (SEQS // 8 - done) // together, group, 0)


def reads(b, head, lo, refs):
    spread, rounded, gain, q_decayed, own_read, heads_out = refs
    together = 8
    low, high = head * LANES, (head + 1) * LANES

    def group(g, carry):
        for unit in range(together):
            s = g * together + unit
            rows = pl.ds(s, SLOTS, stride=SEQS)
            read = dot(q_decayed[head, rows, :].astype(BF16), rounded[s, head])
            read = read + own_read[head, rows, :]
            square = jnp.mean(read * read, axis=1, keepdims=True)
            gate = silu(spread[b, head, 3, rows, :])
            out = read * lax.rsqrt(square + EPSILON) * gain[b : b + 1, low:high] * gate
            heads_out[head, pl.ds(pl.multiple_of(s * SLOTS, SLOTS), SLOTS), :] = out
        return carry

    lax.fori_loop(lo // SLOTS // together, SEQS // together, group, 0)


def round_states(b, states, rounded):
    def group(g, carry):
        rounded[pl.ds(g * 4, 4)] = states[b, pl.ds(g * 4, 4)].astype(BF16)
        return carry

    lax.fori_loop(0, SEQS // 4, group, 0)


def advance_states(b, first, number, refs):
    states, spread, keys, decay_total = refs

    def group(g, carry):
        diagonal = iota((LANES, LANES), 0) == iota((LANES, LANES), 1)
        totals = decay_total[b, pl.ds(pl.multiple_of(g * 8, 8), 8), :]
        for unit in range(8):
            s = g * 8 + unit
            slots = pl.ds(s, SLOTS, stride=SEQS)
            for head in range(HEADS):
                added = dot_rows(
                    keys[b, head, slots, :].astype(BF16), spread[b, head, 2, slots, :].astype(BF16)
                )
                total = totals[unit : unit + 1, head * LANES : (head + 1) * LANES]
                kept = jnp.sum(jnp.where(diagonal, total, 0.0), axis=1, keepdims=True)
                states[b, s, head] = kept * states[b, s, head] + added
        return carry

    lax.fori_loop(first, first + number, group, 0)


def blocks_kernel(pieces, *refs):
    count = len(pieces)
    (spans, act, gain_in, w_q, w_f, w_v, w_g, minimum, extra, gain_out, emission, memory) = refs[:12]
    (rank, many, final_x, states) = refs[12:16]
    refs = list(refs[16:])

    def take(number):
        taken = refs[:number]
        del refs[:number]
        return taken

    (gathered, column, raw, gain_peer, weights, outward, rounded, normed, spread, q_decayed, own_read) = take(11)
    (heads_out, added, keys, decay_total) = take(4)
    (local_sems, swap_send, swap_recv, count_send, count_recv, send_sems, recv_sems) = take(7)
    per = [take(13) for _ in range(count)]
    x, core, z, y = here()
    dp = x * 2 + core

    xs = [device(around(x, o), core, z, y) for o in range(1, RING)]
    ys = [device(x, core, z, around(y, o)) for o in range(1, RING)]
    zs = [device(x, core, around(z, o), y) for o in range(1, RING)]
    crossed = [device(x, 1 - core, around(z, o), y) for o in range(RING)]
    others = [device(around(x, o), 1 - core, z, y) for o in range(1, RING)]
    partner = crossed[0]
    kernels = (w_q, w_f, w_v, w_g)

    local, swaps, sent = [], [], []

    def bring(source, target):
        copy = pltpu.make_async_copy(source, target, local_sems.at[len(local)])
        copy.start()
        local.append(copy)
        return copy

    def swap(source, target):
        number = len(swaps)
        copy = pltpu.make_async_remote_copy(
            source,
            target,
            swap_send.at[number],
            swap_recv.at[number],
            device_id=partner,
            device_id_type=MESH,
        )
        copy.start()
        swaps.append(copy)
        return copy

    def send(b, i, phase, number, source, target, peer):
        copy = pltpu.make_async_remote_copy(
            source,
            target,
            send_sems.at[b, i, phase, number],
            recv_sems.at[b, i, phase, number],
            device_id=peer,
            device_id_type=MESH,
        )
        copy.start()
        sent.append(copy)
        return copy

    def rows_of(side, j):
        return act.at[pl.ds((j * 2 + side) * SHARD_ROWS, SHARD_ROWS), :]

    def weight_parts(b, head, first):
        for k in range(4):
            yield (
                kernels[k].at[b, :, head * LANES : (head + 1) * LANES],
                weights.at[b, head, first : first + FEATURES, k * LANES : (k + 1) * LANES],
            )

    own_rows = [bring(rows_of(core, j), raw.at[j, :, 0:FEATURES]) for j in range(RING)]
    own_weights = [[[bring(*part) for part in weight_parts(0, h, 0)] for h in range(HEADS)]]
    own_states = [bring(memory.at[b], states.at[b]) for b in range(BLOCKS)]
    own_outward = [bring(emission.at[b], outward.at[b, :, 0:FEATURES]) for b in range(BLOCKS)]
    own_weights.append([[bring(*part) for part in weight_parts(1, h, 0)] for h in range(HEADS)])

    greet(xs + ys + zs + crossed + others)

    counts = []
    for number, peer in enumerate(xs + [partner] + others):
        copy = pltpu.make_async_remote_copy(
            spans,
            gathered.at[dp],
            count_send.at[number],
            count_recv.at[number],
            device_id=peer,
            device_id_type=MESH,
        )
        copy.start()
        counts.append(copy)
    peer_rows = [swap(rows_of(1 - core, j), raw.at[j, :, FEATURES : 2 * FEATURES]) for j in range(RING)]
    peer_gain = swap(gain_in, gain_peer)
    peer_weights = [[[swap(*part) for part in weight_parts(0, h, FEATURES)] for h in range(HEADS)]]
    peer_outward = [swap(emission.at[b], outward.at[b, :, FEATURES : 2 * FEATURES]) for b in range(BLOCKS)]
    peer_weights.append([[swap(*part) for part in weight_parts(1, h, FEATURES)] for h in range(HEADS)])

    gathered[dp] = spans[...]
    fill_columns(spans, column)
    for copy in counts:
        copy.wait_recv()
    fill_ranks(gathered, rank, many)
    for j in range(RING):
        own_rows[j].wait()
        peer_rows[j].wait_recv()
    peer_gain.wait_recv()
    waiting = []

    def widen():
        diagonal = iota((LANES, LANES), 0) == iota((LANES, LANES), 1)
        for b in range(BLOCKS):
            for head in range(HEADS):
                for part in range(SHARD_ROWS // LANES):
                    row = extra[b, head : head + 1, part * LANES : (part + 1) * LANES]
                    wide = jnp.sum(jnp.where(diagonal, jnp.exp(row), 0.0), axis=1, keepdims=True)
                    added[b, head, part * LANES : (part + 1) * LANES, :] = jnp.broadcast_to(wide, (LANES, LANES))

    def piece_steps(i):
        first, rows = pieces[i]
        (x_own, x_peer, parts, got, squares, got_squares, heads, u_own, u_peer, one, two_own, two_peer, last_peer) = per[i]
        for j in range(RING):
            picked = dot(chosen(rank[j * 2 + core], first, rows), raw[j]).astype(BF16)
            for part in range(CHUNKS):
                x_own[0, j, part] = picked[:, part * WIDE : (part + 1) * WIDE]
                x_peer[0, j, part] = picked[:, FEATURES + part * WIDE : FEATURES + (part + 1) * WIDE]
        for b in range(BLOCKS):
            wide = max(rows, LANES)
            eye = iota((rows, wide), 0) == iota((rows, wide), 1)
            for j in range(RING):
                at = slice(j * rows, (j + 1) * rows)
                for part in range(CHUNKS):
                    low, high = part * WIDE, (part + 1) * WIDE
                    own = x_own[b, j, part].astype(F32) * gain_in[b : b + 1, low:high]
                    peer = x_peer[b, j, part].astype(F32) * gain_peer[b : b + 1, low:high]
                    normed[at, low:high] = own.astype(BF16)
                    normed[at, FEATURES + low : FEATURES + high] = peer.astype(BF16)
            waits = []
            for head in range(HEADS):
                if i == 0:
                    for k in range(4):
                        own_weights[b][head][k].wait()
                        peer_weights[b][head][k].wait_recv()

                def project(k, carry, b=b, head=head):
                    columns = pl.ds(pl.multiple_of(k * CHANNELS, CHANNELS), CHANNELS)
                    product = dot(normed[0 : RING * rows], weights[b, head, :, columns]).astype(BF16)
                    for j in range(RING):
                        parts[b, head, j, :, columns] = product[j * rows : (j + 1) * rows]
                    return carry

                lax.fori_loop(0, 2, project, 0)
                for o in (2, 1, 3):
                    waits.append(
                        send(
                            b, i, 0, head * RING + o, parts.at[b, head, around(x, o)], got.at[b, head, o - 1], xs[o - 1]
                        )
                    )
            for j in range(RING):
                total = jnp.zeros((rows, 1), F32)
                for part in range(CHUNKS):
                    own = x_own[b, j, part].astype(F32)
                    peer = x_peer[b, j, part].astype(F32)
                    total = total + jnp.sum(own * own + peer * peer, axis=1, keepdims=True)
                squares[b, j] = jnp.sum(jnp.where(eye, total, 0.0), axis=0, keepdims=True)
            square_waits = []
            for o in (2, 1, 3):
                square_waits.append(
                    send(b, i, 1, o, squares.at[b, around(x, o)], got_squares.at[b, o - 1], xs[o - 1])
                )
            if i == count - 1:
                if b == 0:
                    widen()
                own_states[b].wait()
                round_states(b, states, rounded)
            yield

            for wait in square_waits:
                wait.wait_recv()
            square = squares[b, x] + got_squares[b, 0] + got_squares[b, 1] + got_squares[b, 2]
            scale_row = lax.rsqrt(square / D + EPSILON)
            scale = jnp.sum(jnp.where(eye, scale_row, 0.0), axis=1, keepdims=True)
            places = chosen(rank[SHARDS + dp], first, rows)
            picking = chosen(rank[dp], first, rows)
            head_waits = []
            for head in range(HEADS):
                for wait in waits[head * 3 : head * 3 + 3]:
                    wait.wait_recv()

                for part in range(2):
                    columns = slice(part * CHANNELS, (part + 1) * CHANNELS)
                    total = parts[b, head, x, :, columns].astype(F32)
                    for o in range(RING - 1):
                        total = total + got[b, head, o, :, columns].astype(F32)
                    placed = dot_rows(places, (total * scale).astype(BF16))
                    for k in range(2):
                        piece = placed[:, k * LANES : (k + 1) * LANES]
                        if i > 0:
                            piece = piece + spread[b, head, part * 2 + k]
                        spread[b, head, part * 2 + k] = piece
                gates(b, head, first, first + rows, (spread, column, minimum, added, q_decayed, own_read, keys, decay_total))
                reads(b, head, first, (spread, rounded, gain_out, q_decayed, own_read, heads_out))
                heads[b, head, x] = dot(picking, heads_out[head].astype(BF16)).astype(BF16)
                for o in (2, 1, 3):
                    mine = heads.at[b, head, x]
                    head_waits.append(send(b, i, 2, head * RING + o, mine, mine, xs[o - 1]))
            if i == count - 1:
                for g in range(SEQS // 8):
                    waiting.append(
                        functools.partial(advance_states, b, g, 1, (states, spread, keys, decay_total))
                    )
            if i == 0:
                own_outward[b].wait()
                peer_outward[b].wait_recv()
            yield

            for wait in head_waits:
                wait.wait_recv()
            all_heads = jnp.concatenate([heads[b, head].reshape(RING * rows, LANES) for head in range(HEADS)], axis=1)
            waits = []
            for part in range(CHUNKS):
                for half, (target, at, peers) in enumerate(((u_own, y, ys), (u_peer, z, zs))):
                    low = half * FEATURES + part * WIDE
                    product = dot(all_heads, outward[b, :, low : low + WIDE]).astype(BF16)
                    for j in range(RING):
                        target[b, j, part] = product[j * rows : (j + 1) * rows]
                    for o in (2, 1, 3):
                        waits.append(
                            send(
                                b, i, 3 + half, part * RING + o, target.at[b, around(at, o), part],
                                one.at[b, half, o - 1, part], peers[o - 1],
                            )
                        )
            yield

            later = []
            for part in range(CHUNKS):
                for half, (mine, at, slots, own, peers) in enumerate(
                    ((u_own, y, two_own, z, zs), (u_peer, z, two_peer, y, ys))
                ):
                    for wait in waits[:3]:
                        wait.wait_recv()
                    del waits[:3]
                    total = mine[b, at, part].astype(F32)
                    for o in range(RING - 1):
                        total = total + one[b, half, o, part].astype(F32)
                    slots[b, own, part] = total.astype(BF16)
                    place = slots.at[b, own, part]
                    for o in (2, 1, 3):
                        later.append(send(b, i, 5 + half, part * RING + o, place, place, peers[o - 1]))
            waits = later
            yield

            later = []
            for part in range(CHUNKS):
                for half, (slots, old, at) in enumerate(((two_own, x_own, y), (two_peer, x_peer, z))):
                    for wait in waits[:3]:
                        wait.wait_recv()
                    del waits[:3]
                    total = slots[b, 0, part].astype(F32)
                    for o in range(1, RING):
                        total = total + slots[b, o, part].astype(F32)
                    fresh = (old[b, at, part].astype(F32) + total.astype(BF16).astype(F32)).astype(BF16)
                    number = part * RING
                    if b < BLOCKS - 1:
                        old[b + 1, at, part] = fresh
                        place = old.at[b + 1, at, part]
                        peers = ys if half == 0 else zs
                        for o in (2, 1, 3):
                            later.append(send(b, i, 7 + half, number + o, place, place, peers[o - 1]))
                    elif half == 0:
                        final_x[core, y, part, first : first + rows] = fresh
                        place = final_x.at[core, y, part, first : first + rows]
                        for o in (2, 1, 3):
                            later.append(send(b, i, 7, number + o, place, place, ys[o - 1]))
                    else:
                        last_peer[part] = fresh
                        place = final_x.at[core, z, part, first : first + rows]
                        for o in (2, 1, 3, 0):
                            later.append(send(b, i, 8, number + o, last_peer.at[part], place, crossed[o]))
            yield
            for wait in later:
                wait.wait_recv()

    running = [piece_steps(i) for i in range(count)]
    tick = 0
    while running:
        still = []
        for steps in running:
            try:
                next(steps)
                still.append(steps)
            except StopIteration:
                pass
            for _ in range(ADVANCES.get((tick % 5, steps is running[-1]), 0)):
                if waiting:
                    waiting.pop(0)()
        running = still
        tick += 1

    for work in waiting:
        work()
    for copy in counts + swaps + sent:
        copy.wait_send()


def blocks(pieces, *args):
    capacity = sum(rows for _, rows in pieces)
    hbm = pl.BlockSpec(memory_space=pltpu.HBM)
    vmem = pl.BlockSpec(memory_space=pltpu.VMEM)
    scratch = [
        pltpu.VMEM((SHARDS, 1, SEQS), jnp.int32),
        pltpu.VMEM((2 * SEQS, LANES), F32),
        pltpu.VMEM((RING, SHARD_ROWS, 2 * FEATURES), BF16),
        pltpu.VMEM((BLOCKS, FEATURES), F32),
        pltpu.VMEM((BLOCKS, HEADS, 2 * FEATURES, 4 * LANES), BF16),
        pltpu.VMEM((BLOCKS, CHANNELS, 2 * FEATURES), BF16),
        pltpu.VMEM((SEQS, HEADS, LANES, LANES), BF16),
        pltpu.VMEM((RING * max(rows for _, rows in pieces), 2 * FEATURES), BF16),
        pltpu.VMEM((BLOCKS, HEADS, 4, SHARD_ROWS, LANES), F32),
        pltpu.VMEM((HEADS, SHARD_ROWS, LANES), F32),
        pltpu.VMEM((HEADS, SHARD_ROWS, LANES), F32),
        pltpu.VMEM((HEADS, SHARD_ROWS, LANES), F32),
        pltpu.VMEM((BLOCKS, HEADS, SHARD_ROWS, LANES), F32),
        pltpu.VMEM((BLOCKS, HEADS, SHARD_ROWS, LANES), F32),
        pltpu.VMEM((BLOCKS, SEQS, CHANNELS), F32),
        pltpu.SemaphoreType.DMA((24,)),
        pltpu.SemaphoreType.DMA((23,)),
        pltpu.SemaphoreType.DMA((23,)),
        pltpu.SemaphoreType.DMA((SHARDS - 1,)),
        pltpu.SemaphoreType.DMA((SHARDS - 1,)),
        pltpu.SemaphoreType.DMA((BLOCKS, len(pieces), 9, RING * max(HEADS, CHUNKS))),
        pltpu.SemaphoreType.DMA((BLOCKS, len(pieces), 9, RING * max(HEADS, CHUNKS))),
    ]
    for _, rows in pieces:
        scratch += [
            pltpu.VMEM((BLOCKS, RING, CHUNKS, rows, WIDE), BF16),
            pltpu.VMEM((BLOCKS, RING, CHUNKS, rows, WIDE), BF16),
            pltpu.VMEM((BLOCKS, HEADS, RING, rows, 4 * LANES), BF16),
            pltpu.VMEM((BLOCKS, HEADS, RING - 1, rows, 4 * LANES), BF16),
            pltpu.VMEM((BLOCKS, RING, 1, max(rows, LANES)), F32),
            pltpu.VMEM((BLOCKS, RING - 1, 1, max(rows, LANES)), F32),
            pltpu.VMEM((BLOCKS, HEADS, RING, rows, LANES), BF16),
            pltpu.VMEM((BLOCKS, RING, CHUNKS, rows, WIDE), BF16),
            pltpu.VMEM((BLOCKS, RING, CHUNKS, rows, WIDE), BF16),
            pltpu.VMEM((BLOCKS, 2, RING - 1, CHUNKS, rows, WIDE), BF16),
            pltpu.VMEM((BLOCKS, RING, CHUNKS, rows, WIDE), BF16),
            pltpu.VMEM((BLOCKS, RING, CHUNKS, rows, WIDE), BF16),
            pltpu.VMEM((CHUNKS, rows, WIDE), BF16),
        ]
    return pl.pallas_call(
        functools.partial(blocks_kernel, pieces),
        out_shape=(
            jax.ShapeDtypeStruct((2 * SHARDS, 1, SHARD_ROWS), F32),
            jax.ShapeDtypeStruct((1, 1), jnp.int32),
            jax.ShapeDtypeStruct((2, RING, CHUNKS, capacity, WIDE), BF16),
            pltpu.VMEM((BLOCKS, SEQS, HEADS, LANES, LANES), F32),
        ),
        in_specs=[vmem, hbm, vmem] + [hbm] * 4 + [vmem] * 3 + [hbm] * 2,
        out_specs=(vmem, pl.BlockSpec(memory_space=pltpu.SMEM), vmem, vmem),
        scratch_shapes=scratch,
        compiler_params=pltpu.CompilerParams(
            collective_id=len(pieces) + capacity, has_side_effects=True, vmem_limit_bytes=(32 if capacity == CAPACITY else 44) * MIB
        ),
        name="blocks",
    )(*args)


def outputs_kernel(rank, rows, held, act, mixed, states, old, fresh, state_sems, in_sems, out_sems):
    capacity = rows.shape[3]
    shard_rows = [pl.ds(d * SHARD_ROWS, SHARD_ROWS) for d in range(SHARDS)]
    loads = [pltpu.make_async_copy(act.at[shard_rows[d]], old.at[d], in_sems.at[d]) for d in range(SHARDS)]
    for load in loads:
        load.start()
    writes = [pltpu.make_async_copy(held.at[b], states.at[b], state_sems.at[b]) for b in range(BLOCKS)]
    for write in writes:
        write.start()
    for load in loads:
        load.wait()

    def shard(d, carry):
        places = chosen(rank[d], 0, capacity)
        live = dot_rows(places, jnp.ones((capacity, LANES), BF16)) > 0.5
        for chunk in range(CHUNKS):
            spread = dot_rows(places, rows[lax.rem(d, 2), lax.div(d, 2), chunk]).astype(BF16)
            for part in range(WIDE // LANES):
                low = chunk * WIDE + part * LANES
                fresh[d, :, low : low + LANES] = jnp.where(
                    live, spread[:, part * LANES : (part + 1) * LANES], old[d, :, low : low + LANES]
                )
        return carry

    lax.fori_loop(0, SHARDS, shard, 0)
    for d in range(SHARDS):
        write = pltpu.make_async_copy(fresh.at[d], mixed.at[shard_rows[d]], out_sems.at[d])
        write.start()
        writes.append(write)
    for write in writes:
        write.wait()


def write_out(rank, rows, held, act):
    anywhere = pl.BlockSpec(memory_space=pl.ANY)
    vmem = pl.BlockSpec(memory_space=pltpu.VMEM)
    return pl.pallas_call(
        outputs_kernel,
        out_shape=(
            jax.ShapeDtypeStruct(act.shape, BF16),
            jax.ShapeDtypeStruct(held.shape, F32),
        ),
        in_specs=[vmem, vmem, vmem, anywhere],
        out_specs=(anywhere, anywhere),
        scratch_shapes=[
            pltpu.VMEM((SHARDS, SHARD_ROWS, FEATURES), BF16),
            pltpu.VMEM((SHARDS, SHARD_ROWS, FEATURES), BF16),
            pltpu.SemaphoreType.DMA((BLOCKS,)),
            pltpu.SemaphoreType.DMA((SHARDS,)),
            pltpu.SemaphoreType.DMA((SHARDS,)),
        ],
        compiler_params=pltpu.CompilerParams(vmem_limit_bytes=16 * 1024 * 1024),
        name="write_out",
    )(rank, rows, held, act)


CAPACITY = 128
FEW = ((0, 64), (64, 64))
ALL = ((0, 256),)


def local(
    activation_rows,
    fresh_spans,
    entry_rescale_vector,
    probe_kernel,
    retention_kernel,
    content_kernel,
    valve_kernel,
    retention_minimum,
    extra_attenuation,
    channel_rescale_vector,
    emission_kernel,
    memory_grids,
):
    given = (
        fresh_spans.reshape(1, SEQS),
        activation_rows,
        entry_rescale_vector,
        probe_kernel,
        retention_kernel,
        content_kernel,
        valve_kernel,
        retention_minimum,
        jnp.transpose(extra_attenuation, (0, 2, 1)),
        channel_rescale_vector,
        emission_kernel,
        memory_grids,
    )
    rank, many, rows, held = blocks(FEW, *given)
    mixed, states = write_out(rank, rows, held, activation_rows)

    def again(carry):
        rank, _, rows, held = blocks(ALL, *given)
        return (jnp.zeros((), jnp.int32), *write_out(rank, rows, held, activation_rows))

    _, mixed, states = lax.while_loop(lambda carry: carry[0] > 0, again, (many[0, 0], mixed, states))
    return mixed, states


def solution(mesh):
    placed = (
        P(None, "dp"),
        P("dp"),
        P(None, "dp"),
        P(None, "dp", "tp"),
        P(None, "dp", "tp"),
        P(None, "dp", "tp"),
        P(None, "dp", "tp"),
        P(None, "tp"),
        P(None, "dp", "tp"),
        P(None, "tp"),
        P(None, "tp", "dp"),
        P(None, "dp", "tp", None, None),
    )
    return jax.shard_map(
        local,
        mesh=mesh,
        in_specs=placed,
        out_specs=(P(None, "dp"), P(None, "dp", "tp", None, None)),
        check_vma=False,
    )
```

```python
import functools

import jax
import jax.numpy as jnp
from jax import lax
from jax.experimental import pallas as pl
from jax.experimental.pallas import tpu as pltpu
from jax.sharding import PartitionSpec as P

D = 4096
BLOCKS = 2
EPSILON = 1e-05
RING = 4
SHARDS = 8
SEQS = 32
SLOTS = 8
SHARD_ROWS = SEQS * SLOTS
FEATURES = 512
CHANNELS = 256
HEADS = 2
LANES = 128
MESH = pl.DeviceIdType.MESH
F32 = jnp.float32
BF16 = jnp.bfloat16
CHUNKS = 2
ADVANCES = {(2, False): 3, (2, True): 1, (3, False): 1, (3, True): 1, (4, False): 1, (4, True): 1}
WIDE = FEATURES // CHUNKS
MIB = 1024 * 1024


def here():
    dp, tp = lax.axis_index("dp"), lax.axis_index("tp")
    return lax.div(dp, 2), lax.rem(dp, 2), lax.div(tp, RING), lax.rem(tp, RING)


def device(x, core, z, y):
    return {"tp": z * RING + y, "dp": x * 2 + core}


def around(index, offset):
    return lax.rem(index + offset, RING)


def greet(peers):
    barrier = pltpu.get_barrier_semaphore()
    for peer in peers:
        pl.semaphore_signal(barrier, inc=1, device_id=peer, device_id_type=MESH)
    pl.semaphore_wait(barrier, len(peers))


def iota(shape, dim):
    return lax.broadcasted_iota(jnp.int32, shape, dim)


def dot(a, b):
    return jnp.dot(a, b, preferred_element_type=F32)


def dot_rows(a, b):
    return lax.dot_general(a, b, (((0,), (0,)), ((), ())), preferred_element_type=F32)


def chosen(rank_row, first, count):
    wanted = (iota((count, rank_row.shape[1]), 0) + first).astype(F32)
    return jnp.where(wanted == rank_row, 1.0, 0.0).astype(BF16)


def fill_columns(spans, column):
    own = spans[...].astype(F32)
    lane, row = iota((SEQS, SEQS), 1), iota((SEQS, SEQS), 0)
    before = jnp.sum(jnp.where(lane < row, own, 0.0), axis=1, keepdims=True)
    same = jnp.sum(jnp.where(lane == row, own, 0.0), axis=1, keepdims=True)
    column[0:SEQS, :] = jnp.broadcast_to(before, (SEQS, LANES))
    column[SEQS:, :] = jnp.broadcast_to(same, (SEQS, LANES))


def fill_ranks(gathered, rank, many):
    spans_all = jnp.concatenate([gathered[index] for index in range(SHARDS)], axis=0).astype(F32)
    most = jnp.max(jnp.sum(spans_all, axis=1, keepdims=True))
    many[0, 0] = jnp.where(most > CAPACITY, 1, 0)
    spans_all = spans_all.astype(BF16)
    slot_index = iota((SEQS, SHARD_ROWS), 1)
    sequence = iota((SEQS, SHARD_ROWS), 0)
    for order in range(2):
        if order == 0:
            owner, position = lax.shift_right_logical(slot_index, 3), slot_index & 7
        else:
            owner, position = slot_index & 31, lax.shift_right_logical(slot_index, 5)
        earlier = jnp.where(sequence < owner, 1.0, 0.0).astype(BF16)
        equal = jnp.where(sequence == owner, 1.0, 0.0).astype(BF16)
        start, length = dot(spans_all, earlier), dot(spans_all, equal)
        place = position[0:SHARDS].astype(F32)
        ranks = jnp.where(place < length, start + place, -1.0)
        for index in range(SHARDS):
            rank[order * SHARDS + index] = ranks[index : index + 1]


def silu(a):
    return a * jax.nn.sigmoid(a)


def gates(b, head, lo, hi, refs):
    spread, column, minimum, added, q_decayed, own_read, keys, decay_total = refs
    ones = jnp.ones((LANES, LANES), BF16)
    low, high = head * LANES, (head + 1) * LANES
    done = lo // SLOTS // 8
    together = 2 if (SEQS // 8 - done) % 2 == 0 else 3

    def group(pair, carry):
        for unit in range(together):
            g = done + pair * together + unit
            start = column[pl.ds(pl.multiple_of(g * 8, 8), 8), :]
            span = column[pl.ds(pl.multiple_of(SEQS + g * 8, 8), 8), :]
            floor = minimum[b : b + 1, low:high]
            kept, values, products = [], [], []
            running = None
            for p in range(SLOTS):
                rows = pl.ds(pl.multiple_of(p * SEQS + g * 8, 8), 8)
                q = silu(spread[b, head, 0, rows, :])
                f = spread[b, head, 1, rows, :]
                values.append(spread[b, head, 2, rows, :])
                small = jnp.exp(-jnp.abs(f))
                large = 1.0 / (1.0 + small)
                small = small * large
                up = f >= 0.0
                live = jnp.logical_and(span > p, start + p < hi)
                forget = floor + (1.0 - floor) * jnp.where(up, large, small)
                decay = jnp.where(live, forget * added[b, head, pl.ds(g * 64 + p, 8, stride=8), :], 1.0)
                key = jnp.where(live, (1.0 - floor) * jnp.where(up, small, large), 0.0)
                running = decay if p == 0 else running * decay
                kept = [old * decay for old in kept] + [key]
                products += [q * old for old in kept]
                q_decayed[head, rows, :] = q * running
            for p in range(SLOTS):
                rows = pl.ds(pl.multiple_of(p * SEQS + g * 8, 8), 8)
                keys[b, head, rows, :] = kept[p]
            decay_total[b, pl.ds(pl.multiple_of(g * 8, 8), 8), low:high] = running
            scores = dot(jnp.concatenate(products, axis=0).astype(BF16), ones)
            number = 0
            for p in range(SLOTS):
                read = None
                for value in values[: p + 1]:
                    term = scores[number * 8 : (number + 1) * 8] * value
                    read = term if read is None else read + term
                    number += 1
                own_read[head, pl.ds(pl.multiple_of(p * SEQS + g * 8, 8), 8), :] = read
        return carry

    lax.fori_loop(0, (SEQS // 8 - done) // together, group, 0)


def reads(b, head, lo, refs):
    spread, rounded, gain, q_decayed, own_read, heads_out = refs
    together = 8
    low, high = head * LANES, (head + 1) * LANES

    def group(g, carry):
        for unit in range(together):
            s = g * together + unit
            rows = pl.ds(s, SLOTS, stride=SEQS)
            read = dot(q_decayed[head, rows, :].astype(BF16), rounded[s, head])
            read = read + own_read[head, rows, :]
            square = jnp.mean(read * read, axis=1, keepdims=True)
            gate = silu(spread[b, head, 3, rows, :])
            out = read * lax.rsqrt(square + EPSILON) * gain[b : b + 1, low:high] * gate
            heads_out[head, pl.ds(pl.multiple_of(s * SLOTS, SLOTS), SLOTS), :] = out
        return carry

    lax.fori_loop(lo // SLOTS // together, SEQS // together, group, 0)


def round_states(b, states, rounded):
    def group(g, carry):
        rounded[pl.ds(g * 4, 4)] = states[b, pl.ds(g * 4, 4)].astype(BF16)
        return carry

    lax.fori_loop(0, SEQS // 4, group, 0)


def advance_states(b, first, number, refs):
    states, spread, keys, decay_total = refs

    def group(g, carry):
        diagonal = iota((LANES, LANES), 0) == iota((LANES, LANES), 1)
        totals = decay_total[b, pl.ds(pl.multiple_of(g * 8, 8), 8), :]
        for unit in range(8):
            s = g * 8 + unit
            slots = pl.ds(s, SLOTS, stride=SEQS)
            for head in range(HEADS):
                added = dot_rows(
                    keys[b, head, slots, :].astype(BF16), spread[b, head, 2, slots, :].astype(BF16)
                )
                total = totals[unit : unit + 1, head * LANES : (head + 1) * LANES]
                kept = jnp.sum(jnp.where(diagonal, total, 0.0), axis=1, keepdims=True)
                states[b, s, head] = kept * states[b, s, head] + added
        return carry

    lax.fori_loop(first, first + number, group, 0)


def blocks_kernel(pieces, *refs):
    count = len(pieces)
    (spans, act, gain_in, w_q, w_f, w_v, w_g, minimum, extra, gain_out, emission, memory) = refs[:12]
    (rank, many, final_x, states) = refs[12:16]
    refs = list(refs[16:])

    def take(number):
        taken = refs[:number]
        del refs[:number]
        return taken

    (gathered, column, raw, gain_peer, weights, outward, rounded, normed, spread, q_decayed, own_read) = take(11)
    (heads_out, added, keys, decay_total) = take(4)
    (local_sems, swap_send, swap_recv, count_send, count_recv, send_sems, recv_sems) = take(7)
    per = [take(13) for _ in range(count)]
    x, core, z, y = here()
    dp = x * 2 + core

    xs = [device(around(x, o), core, z, y) for o in range(1, RING)]
    ys = [device(x, core, z, around(y, o)) for o in range(1, RING)]
    zs = [device(x, core, around(z, o), y) for o in range(1, RING)]
    crossed = [device(x, 1 - core, around(z, o), y) for o in range(RING)]
    others = [device(around(x, o), 1 - core, z, y) for o in range(1, RING)]
    partner = crossed[0]
    kernels = (w_q, w_f, w_v, w_g)

    local, swaps, sent = [], [], []

    def bring(source, target):
        copy = pltpu.make_async_copy(source, target, local_sems.at[len(local)])
        copy.start()
        local.append(copy)
        return copy

    def swap(source, target):
        number = len(swaps)
        copy = pltpu.make_async_remote_copy(
            source,
            target,
            swap_send.at[number],
            swap_recv.at[number],
            device_id=partner,
            device_id_type=MESH,
        )
        copy.start()
        swaps.append(copy)
        return copy

    def scatter(b, i, phase, number, copies, sources, targets):
        send_sem, recv_sem = send_sems.at[b, i, phase, number], recv_sems.at[b, i, phase, number]
        for source, target, peer in copies:
            pltpu.make_async_remote_copy(
                source, target, send_sem, recv_sem, device_id=peer, device_id_type=MESH
            ).start()
        sent.append(pltpu.make_async_copy(sources, sources, send_sem))
        return pltpu.make_async_copy(targets, targets, recv_sem)

    def rows_of(side, j):
        return act.at[pl.ds((j * 2 + side) * SHARD_ROWS, SHARD_ROWS), :]

    def weight_parts(b, head, first):
        for k in range(4):
            yield (
                kernels[k].at[b, :, head * LANES : (head + 1) * LANES],
                weights.at[b, head, first : first + FEATURES, k * LANES : (k + 1) * LANES],
            )

    own_rows = [bring(rows_of(core, j), raw.at[j, :, 0:FEATURES]) for j in range(RING)]
    own_weights = [[[bring(*part) for part in weight_parts(0, h, 0)] for h in range(HEADS)]]
    own_states = [bring(memory.at[b], states.at[b]) for b in range(BLOCKS)]
    own_outward = [bring(emission.at[b], outward.at[b, :, 0:FEATURES]) for b in range(BLOCKS)]
    own_weights.append([[bring(*part) for part in weight_parts(1, h, 0)] for h in range(HEADS)])

    greet(xs + ys + zs + crossed + others)

    counts = []
    for number, peer in enumerate(xs + [partner] + others):
        copy = pltpu.make_async_remote_copy(
            spans,
            gathered.at[dp],
            count_send.at[number],
            count_recv.at[number],
            device_id=peer,
            device_id_type=MESH,
        )
        copy.start()
        counts.append(copy)
    peer_rows = [swap(rows_of(1 - core, j), raw.at[j, :, FEATURES : 2 * FEATURES]) for j in range(RING)]
    peer_gain = swap(gain_in, gain_peer)
    peer_weights = [[[swap(*part) for part in weight_parts(0, h, FEATURES)] for h in range(HEADS)]]
    peer_outward = [swap(emission.at[b], outward.at[b, :, FEATURES : 2 * FEATURES]) for b in range(BLOCKS)]
    peer_weights.append([[swap(*part) for part in weight_parts(1, h, FEATURES)] for h in range(HEADS)])

    gathered[dp] = spans[...]
    fill_columns(spans, column)
    for copy in counts:
        copy.wait_recv()
    fill_ranks(gathered, rank, many)
    for j in range(RING):
        own_rows[j].wait()
        peer_rows[j].wait_recv()
    peer_gain.wait_recv()
    waiting = []

    def widen():
        diagonal = iota((LANES, LANES), 0) == iota((LANES, LANES), 1)
        for b in range(BLOCKS):
            for head in range(HEADS):
                for part in range(SHARD_ROWS // LANES):
                    row = extra[b, head : head + 1, part * LANES : (part + 1) * LANES]
                    wide = jnp.sum(jnp.where(diagonal, jnp.exp(row), 0.0), axis=1, keepdims=True)
                    added[b, head, part * LANES : (part + 1) * LANES, :] = jnp.broadcast_to(wide, (LANES, LANES))

    def piece_steps(i):
        first, rows = pieces[i]
        (x_own, x_peer, parts, got, squares, got_squares, heads, u_own, u_peer, one, two_own, two_peer, last_peer) = per[i]
        for j in range(RING):
            picked = dot(chosen(rank[j * 2 + core], first, rows), raw[j]).astype(BF16)
            for part in range(CHUNKS):
                x_own[0, part, j] = picked[:, part * WIDE : (part + 1) * WIDE]
                x_peer[0, part, j] = picked[:, FEATURES + part * WIDE : FEATURES + (part + 1) * WIDE]
        for b in range(BLOCKS):
            wide = max(rows, LANES)
            eye = iota((rows, wide), 0) == iota((rows, wide), 1)
            for j in range(RING):
                total = jnp.zeros((rows, 1), F32)
                for part in range(CHUNKS):
                    own = x_own[b, part, j].astype(F32)
                    peer = x_peer[b, part, j].astype(F32)
                    total = total + jnp.sum(own * own + peer * peer, axis=1, keepdims=True)
                squares[b, j] = jnp.sum(jnp.where(eye, total, 0.0), axis=0, keepdims=True)
            square_wait = scatter(
                b, i, 0, 0,
                [(squares.at[b, around(x, o)], got_squares.at[b, o - 1], xs[o - 1]) for o in (2, 1, 3)],
                squares.at[b, 0:3], got_squares.at[b],
            )
            for j in range(RING):
                at = slice(j * rows, (j + 1) * rows)
                for part in range(CHUNKS):
                    low, high = part * WIDE, (part + 1) * WIDE
                    own = x_own[b, part, j].astype(F32) * gain_in[b : b + 1, low:high]
                    peer = x_peer[b, part, j].astype(F32) * gain_peer[b : b + 1, low:high]
                    normed[at, low:high] = own.astype(BF16)
                    normed[at, FEATURES + low : FEATURES + high] = peer.astype(BF16)
            waits = []
            for head in range(HEADS):
                if i == 0:
                    for k in range(4):
                        own_weights[b][head][k].wait()
                        peer_weights[b][head][k].wait_recv()

                def project(k, carry, b=b, head=head):
                    columns = pl.ds(pl.multiple_of(k * CHANNELS, CHANNELS), CHANNELS)
                    product = dot(normed[0 : RING * rows], weights[b, head, :, columns]).astype(BF16)
                    for j in range(RING):
                        parts[b, head, j, :, columns] = product[j * rows : (j + 1) * rows]
                    return carry

                lax.fori_loop(0, 2, project, 0)
                waits.append(
                    scatter(
                        b, i, 1, head,
                        [(parts.at[b, head, around(x, o)], got.at[b, head, o - 1], xs[o - 1]) for o in (2, 1, 3)],
                        parts.at[b, head, 0:3], got.at[b, head],
                    )
                )
            if i == count - 1:
                if b == 0:
                    widen()
                own_states[b].wait()
                round_states(b, states, rounded)
            yield

            square_wait.wait()
            square = squares[b, x] + got_squares[b, 0] + got_squares[b, 1] + got_squares[b, 2]
            scale_row = lax.rsqrt(square / D + EPSILON)
            scale = jnp.sum(jnp.where(eye, scale_row, 0.0), axis=1, keepdims=True)
            places = chosen(rank[SHARDS + dp], first, rows)
            picking = chosen(rank[dp], first, rows)
            head_waits = []
            for head in range(HEADS):
                waits[head].wait()

                for part in range(2):
                    columns = slice(part * CHANNELS, (part + 1) * CHANNELS)
                    total = parts[b, head, x, :, columns].astype(F32)
                    for o in range(RING - 1):
                        total = total + got[b, head, o, :, columns].astype(F32)
                    placed = dot_rows(places, (total * scale).astype(BF16))
                    for k in range(2):
                        piece = placed[:, k * LANES : (k + 1) * LANES]
                        if i > 0:
                            piece = piece + spread[b, head, part * 2 + k]
                        spread[b, head, part * 2 + k] = piece
                gates(b, head, first, first + rows, (spread, column, minimum, added, q_decayed, own_read, keys, decay_total))
                reads(b, head, first, (spread, rounded, gain_out, q_decayed, own_read, heads_out))
                heads[b, head, x] = dot(picking, heads_out[head].astype(BF16)).astype(BF16)
                mine, three = heads.at[b, head, x], heads.at[b, head, 0:3]
                head_waits.append(
                    scatter(b, i, 2, head, [(mine, mine, xs[o - 1]) for o in (2, 1, 3)], three, three)
                )
            if i == count - 1:
                for g in range(SEQS // 8):
                    waiting.append(
                        functools.partial(advance_states, b, g, 1, (states, spread, keys, decay_total))
                    )
            if i == 0:
                own_outward[b].wait()
                peer_outward[b].wait_recv()
            yield

            for wait in head_waits:
                wait.wait()
            all_heads = jnp.concatenate([heads[b, head].reshape(RING * rows, LANES) for head in range(HEADS)], axis=1)
            waits = []
            for part in range(CHUNKS):
                for half, (target, at, peers) in enumerate(((u_own, y, ys), (u_peer, z, zs))):
                    low = half * FEATURES + part * WIDE
                    product = dot(all_heads, outward[b, :, low : low + WIDE]).astype(BF16)
                    for j in range(RING):
                        target[b, part, j] = product[j * rows : (j + 1) * rows]
                    waits.append(
                        scatter(
                            b, i, 3 + half, part,
                            [
                                (target.at[b, part, around(at, o)], one.at[b, half, part, o - 1], peers[o - 1])
                                for o in (2, 1, 3)
                            ],
                            target.at[b, part, 0:3], one.at[b, half, part],
                        )
                    )
            yield

            later = []
            for part in range(CHUNKS):
                for half, (mine, at, slots, own, peers) in enumerate(
                    ((u_own, y, two_own, z, zs), (u_peer, z, two_peer, y, ys))
                ):
                    waits.pop(0).wait()
                    total = mine[b, part, at].astype(F32)
                    for o in range(RING - 1):
                        total = total + one[b, half, part, o].astype(F32)
                    slots[b, part, own] = total.astype(BF16)
                    place, three = slots.at[b, part, own], slots.at[b, part, 0:3]
                    later.append(
                        scatter(b, i, 5 + half, part, [(place, place, peers[o - 1]) for o in (2, 1, 3)], three, three)
                    )
            waits = later
            yield

            later = []
            for part in range(CHUNKS):
                for half, (slots, old, at) in enumerate(((two_own, x_own, y), (two_peer, x_peer, z))):
                    waits.pop(0).wait()
                    total = slots[b, part, 0].astype(F32)
                    for o in range(1, RING):
                        total = total + slots[b, part, o].astype(F32)
                    fresh = (old[b, part, at].astype(F32) + total.astype(BF16).astype(F32)).astype(BF16)
                    within = slice(first, first + rows)
                    if b < BLOCKS - 1:
                        old[b + 1, part, at] = fresh
                        place, three = old.at[b + 1, part, at], old.at[b + 1, part, 0:3]
                        peers = ys if half == 0 else zs
                        copies = [(place, place, peers[o - 1]) for o in (2, 1, 3)]
                        later.append(scatter(b, i, 7 + half, part, copies, three, three))
                    elif half == 0:
                        final_x[core, part, y, within] = fresh
                        place, three = final_x.at[core, part, y, within], final_x.at[core, part, 0:3, within]
                        copies = [(place, place, ys[o - 1]) for o in (2, 1, 3)]
                        later.append(scatter(b, i, 7, part, copies, three, three))
                    else:
                        last_peer[part] = fresh
                        place, four = final_x.at[core, part, z, within], final_x.at[1 - core, part, 0:4, within]
                        copies = [(last_peer.at[part], place, crossed[o]) for o in (2, 1, 3, 0)]
                        later.append(scatter(b, i, 8, part, copies, four, four))
            yield
            for wait in later:
                wait.wait()

    running = [piece_steps(i) for i in range(count)]
    tick, aged = 0, []
    while running:
        still = []
        for steps in running:
            try:
                next(steps)
                still.append(steps)
            except StopIteration:
                pass
            for _ in range(ADVANCES.get((tick % 5, steps is running[-1]), 0)):
                if waiting:
                    waiting.pop(0)()
        for copy in aged:
            copy.wait()
        aged = list(sent)
        sent.clear()
        if tick == 1:
            for copy in swaps + counts:
                copy.wait_send()
        running = still
        tick += 1

    for work in waiting:
        work()
    for copy in aged + sent:
        copy.wait()


def blocks(pieces, *args):
    capacity = sum(rows for _, rows in pieces)
    hbm = pl.BlockSpec(memory_space=pltpu.HBM)
    vmem = pl.BlockSpec(memory_space=pltpu.VMEM)
    scratch = [
        pltpu.VMEM((SHARDS, 1, SEQS), jnp.int32),
        pltpu.VMEM((2 * SEQS, LANES), F32),
        pltpu.VMEM((RING, SHARD_ROWS, 2 * FEATURES), BF16),
        pltpu.VMEM((BLOCKS, FEATURES), F32),
        pltpu.VMEM((BLOCKS, HEADS, 2 * FEATURES, 4 * LANES), BF16),
        pltpu.VMEM((BLOCKS, CHANNELS, 2 * FEATURES), BF16),
        pltpu.VMEM((SEQS, HEADS, LANES, LANES), BF16),
        pltpu.VMEM((RING * max(rows for _, rows in pieces), 2 * FEATURES), BF16),
        pltpu.VMEM((BLOCKS, HEADS, 4, SHARD_ROWS, LANES), F32),
        pltpu.VMEM((HEADS, SHARD_ROWS, LANES), F32),
        pltpu.VMEM((HEADS, SHARD_ROWS, LANES), F32),
        pltpu.VMEM((HEADS, SHARD_ROWS, LANES), F32),
        pltpu.VMEM((BLOCKS, HEADS, SHARD_ROWS, LANES), F32),
        pltpu.VMEM((BLOCKS, HEADS, SHARD_ROWS, LANES), F32),
        pltpu.VMEM((BLOCKS, SEQS, CHANNELS), F32),
        pltpu.SemaphoreType.DMA((24,)),
        pltpu.SemaphoreType.DMA((23,)),
        pltpu.SemaphoreType.DMA((23,)),
        pltpu.SemaphoreType.DMA((SHARDS - 1,)),
        pltpu.SemaphoreType.DMA((SHARDS - 1,)),
        pltpu.SemaphoreType.DMA((BLOCKS, len(pieces), 9, max(HEADS, CHUNKS))),
        pltpu.SemaphoreType.DMA((BLOCKS, len(pieces), 9, max(HEADS, CHUNKS))),
    ]
    for _, rows in pieces:
        scratch += [
            pltpu.VMEM((BLOCKS, CHUNKS, RING, rows, WIDE), BF16),
            pltpu.VMEM((BLOCKS, CHUNKS, RING, rows, WIDE), BF16),
            pltpu.VMEM((BLOCKS, HEADS, RING, rows, 4 * LANES), BF16),
            pltpu.VMEM((BLOCKS, HEADS, RING - 1, rows, 4 * LANES), BF16),
            pltpu.VMEM((BLOCKS, RING, 1, max(rows, LANES)), F32),
            pltpu.VMEM((BLOCKS, RING - 1, 1, max(rows, LANES)), F32),
            pltpu.VMEM((BLOCKS, HEADS, RING, rows, LANES), BF16),
            pltpu.VMEM((BLOCKS, CHUNKS, RING, rows, WIDE), BF16),
            pltpu.VMEM((BLOCKS, CHUNKS, RING, rows, WIDE), BF16),
            pltpu.VMEM((BLOCKS, 2, CHUNKS, RING - 1, rows, WIDE), BF16),
            pltpu.VMEM((BLOCKS, CHUNKS, RING, rows, WIDE), BF16),
            pltpu.VMEM((BLOCKS, CHUNKS, RING, rows, WIDE), BF16),
            pltpu.VMEM((CHUNKS, rows, WIDE), BF16),
        ]
    return pl.pallas_call(
        functools.partial(blocks_kernel, pieces),
        out_shape=(
            jax.ShapeDtypeStruct((2 * SHARDS, 1, SHARD_ROWS), F32),
            jax.ShapeDtypeStruct((1, 1), jnp.int32),
            jax.ShapeDtypeStruct((2, CHUNKS, RING, capacity, WIDE), BF16),
            pltpu.VMEM((BLOCKS, SEQS, HEADS, LANES, LANES), F32),
        ),
        in_specs=[vmem, hbm, vmem] + [hbm] * 4 + [vmem] * 3 + [hbm] * 2,
        out_specs=(vmem, pl.BlockSpec(memory_space=pltpu.SMEM), vmem, vmem),
        scratch_shapes=scratch,
        compiler_params=pltpu.CompilerParams(
            collective_id=len(pieces) + capacity, has_side_effects=True, vmem_limit_bytes=(32 if capacity == CAPACITY else 44) * MIB
        ),
        name="blocks",
    )(*args)


def outputs_kernel(rank, rows, held, act, mixed, states, old, fresh, state_sems, in_sems, out_sems):
    capacity = rows.shape[3]
    shard_rows = [pl.ds(d * SHARD_ROWS, SHARD_ROWS) for d in range(SHARDS)]
    loads = [pltpu.make_async_copy(act.at[shard_rows[d]], old.at[d], in_sems.at[d]) for d in range(SHARDS)]
    for load in loads:
        load.start()
    writes = [pltpu.make_async_copy(held.at[b], states.at[b], state_sems.at[b]) for b in range(BLOCKS)]
    for write in writes:
        write.start()
    for load in loads:
        load.wait()

    def shard(d, carry):
        places = chosen(rank[d], 0, capacity)
        live = dot_rows(places, jnp.ones((capacity, LANES), BF16)) > 0.5
        for chunk in range(CHUNKS):
            spread = dot_rows(places, rows[lax.rem(d, 2), chunk, lax.div(d, 2)]).astype(BF16)
            for part in range(WIDE // LANES):
                low = chunk * WIDE + part * LANES
                fresh[d, :, low : low + LANES] = jnp.where(
                    live, spread[:, part * LANES : (part + 1) * LANES], old[d, :, low : low + LANES]
                )
        return carry

    lax.fori_loop(0, SHARDS, shard, 0)
    for d in range(SHARDS):
        write = pltpu.make_async_copy(fresh.at[d], mixed.at[shard_rows[d]], out_sems.at[d])
        write.start()
        writes.append(write)
    for write in writes:
        write.wait()


def write_out(rank, rows, held, act):
    anywhere = pl.BlockSpec(memory_space=pl.ANY)
    vmem = pl.BlockSpec(memory_space=pltpu.VMEM)
    return pl.pallas_call(
        outputs_kernel,
        out_shape=(
            jax.ShapeDtypeStruct(act.shape, BF16),
            jax.ShapeDtypeStruct(held.shape, F32),
        ),
        in_specs=[vmem, vmem, vmem, anywhere],
        out_specs=(anywhere, anywhere),
        scratch_shapes=[
            pltpu.VMEM((SHARDS, SHARD_ROWS, FEATURES), BF16),
            pltpu.VMEM((SHARDS, SHARD_ROWS, FEATURES), BF16),
            pltpu.SemaphoreType.DMA((BLOCKS,)),
            pltpu.SemaphoreType.DMA((SHARDS,)),
            pltpu.SemaphoreType.DMA((SHARDS,)),
        ],
        compiler_params=pltpu.CompilerParams(vmem_limit_bytes=16 * 1024 * 1024),
        name="write_out",
    )(rank, rows, held, act)


CAPACITY = 128
FEW = ((0, 64), (64, 64))
ALL = ((0, 256),)


def local(
    activation_rows,
    fresh_spans,
    entry_rescale_vector,
    probe_kernel,
    retention_kernel,
    content_kernel,
    valve_kernel,
    retention_minimum,
    extra_attenuation,
    channel_rescale_vector,
    emission_kernel,
    memory_grids,
):
    given = (
        fresh_spans.reshape(1, SEQS),
        activation_rows,
        entry_rescale_vector,
        probe_kernel,
        retention_kernel,
        content_kernel,
        valve_kernel,
        retention_minimum,
        jnp.transpose(extra_attenuation, (0, 2, 1)),
        channel_rescale_vector,
        emission_kernel,
        memory_grids,
    )
    rank, many, rows, held = blocks(FEW, *given)
    mixed, states = write_out(rank, rows, held, activation_rows)

    def again(carry):
        rank, _, rows, held = blocks(ALL, *given)
        return (jnp.zeros((), jnp.int32), *write_out(rank, rows, held, activation_rows))

    _, mixed, states = lax.while_loop(lambda carry: carry[0] > 0, again, (many[0, 0], mixed, states))
    return mixed, states


def solution(mesh):
    placed = (
        P(None, "dp"),
        P("dp"),
        P(None, "dp"),
        P(None, "dp", "tp"),
        P(None, "dp", "tp"),
        P(None, "dp", "tp"),
        P(None, "dp", "tp"),
        P(None, "tp"),
        P(None, "dp", "tp"),
        P(None, "tp"),
        P(None, "tp", "dp"),
        P(None, "dp", "tp", None, None),
    )
    return jax.shard_map(
        local,
        mesh=mesh,
        in_specs=placed,
        out_specs=(P(None, "dp"), P(None, "dp", "tp", None, None)),
        check_vma=False,
    )
```

```python
import functools

import jax
import jax.numpy as jnp
from jax import lax
from jax.experimental import pallas as pl
from jax.experimental.pallas import tpu as pltpu
from jax.sharding import PartitionSpec as P

D = 4096
BLOCKS = 2
EPSILON = 1e-05
RING = 4
SHARDS = 8
SEQS = 32
SLOTS = 8
SHARD_ROWS = SEQS * SLOTS
FEATURES = 512
CHANNELS = 256
HEADS = 2
LANES = 128
MESH = pl.DeviceIdType.MESH
F32 = jnp.float32
BF16 = jnp.bfloat16
CHUNKS = 2
ADVANCES = {(2, False): 3, (2, True): 1, (3, False): 1, (3, True): 1, (4, False): 1, (4, True): 1}
WIDE = FEATURES // CHUNKS
MIB = 1024 * 1024


def here():
    dp, tp = lax.axis_index("dp"), lax.axis_index("tp")
    return lax.div(dp, 2), lax.rem(dp, 2), lax.div(tp, RING), lax.rem(tp, RING)


def device(x, core, z, y):
    return {"tp": z * RING + y, "dp": x * 2 + core}


def around(index, offset):
    return lax.rem(index + offset, RING)


def greet(peers):
    barrier = pltpu.get_barrier_semaphore()
    for peer in peers:
        pl.semaphore_signal(barrier, inc=1, device_id=peer, device_id_type=MESH)
    pl.semaphore_wait(barrier, len(peers))


def iota(shape, dim):
    return lax.broadcasted_iota(jnp.int32, shape, dim)


def dot(a, b):
    return jnp.dot(a, b, preferred_element_type=F32)


def dot_rows(a, b):
    return lax.dot_general(a, b, (((0,), (0,)), ((), ())), preferred_element_type=F32)


def chosen(rank_row, first, count):
    wanted = (iota((count, rank_row.shape[1]), 0) + first).astype(F32)
    return jnp.where(wanted == rank_row, 1.0, 0.0).astype(BF16)


def fill_columns(spans, column):
    own = spans[...].astype(F32)
    lane, row = iota((SEQS, SEQS), 1), iota((SEQS, SEQS), 0)
    before = jnp.sum(jnp.where(lane < row, own, 0.0), axis=1, keepdims=True)
    same = jnp.sum(jnp.where(lane == row, own, 0.0), axis=1, keepdims=True)
    column[0:SEQS, :] = jnp.broadcast_to(before, (SEQS, LANES))
    column[SEQS:, :] = jnp.broadcast_to(same, (SEQS, LANES))


def fill_ranks(gathered, rank, many):
    spans_all = jnp.concatenate([gathered[index] for index in range(SHARDS)], axis=0).astype(F32)
    most = jnp.max(jnp.sum(spans_all, axis=1, keepdims=True))
    many[0, 0] = jnp.where(most > CAPACITY, 1, 0)
    spans_all = spans_all.astype(BF16)
    slot_index = iota((SEQS, SHARD_ROWS), 1)
    sequence = iota((SEQS, SHARD_ROWS), 0)
    for order in range(2):
        if order == 0:
            owner, position = lax.shift_right_logical(slot_index, 3), slot_index & 7
        else:
            owner, position = slot_index & 31, lax.shift_right_logical(slot_index, 5)
        earlier = jnp.where(sequence < owner, 1.0, 0.0).astype(BF16)
        equal = jnp.where(sequence == owner, 1.0, 0.0).astype(BF16)
        start, length = dot(spans_all, earlier), dot(spans_all, equal)
        place = position[0:SHARDS].astype(F32)
        ranks = jnp.where(place < length, start + place, -1.0)
        for index in range(SHARDS):
            rank[order * SHARDS + index] = ranks[index : index + 1]


def silu(a):
    return a * jax.nn.sigmoid(a)


def gates(b, head, lo, hi, refs):
    spread, column, minimum, added, q_decayed, own_read, keys, decay_total = refs
    ones = jnp.ones((LANES, LANES), BF16)
    low, high = head * LANES, (head + 1) * LANES
    done = lo // SLOTS // 8
    together = 2 if (SEQS // 8 - done) % 2 == 0 else 3

    def group(pair, carry):
        for unit in range(together):
            g = done + pair * together + unit
            start = column[pl.ds(pl.multiple_of(g * 8, 8), 8), :]
            span = column[pl.ds(pl.multiple_of(SEQS + g * 8, 8), 8), :]
            floor = minimum[b : b + 1, low:high]
            kept, values, products = [], [], []
            running = None
            for p in range(SLOTS):
                rows = pl.ds(pl.multiple_of(p * SEQS + g * 8, 8), 8)
                q = silu(spread[b, head, 0, rows, :])
                f = spread[b, head, 1, rows, :]
                values.append(spread[b, head, 2, rows, :])
                small = jnp.exp(-jnp.abs(f))
                large = 1.0 / (1.0 + small)
                small = small * large
                up = f >= 0.0
                live = jnp.logical_and(span > p, start + p < hi)
                forget = floor + (1.0 - floor) * jnp.where(up, large, small)
                decay = jnp.where(live, forget * added[b, head, pl.ds(g * 64 + p, 8, stride=8), :], 1.0)
                key = jnp.where(live, (1.0 - floor) * jnp.where(up, small, large), 0.0)
                running = decay if p == 0 else running * decay
                kept = [old * decay for old in kept] + [key]
                products += [q * old for old in kept]
                q_decayed[head, rows, :] = q * running
            for p in range(SLOTS):
                rows = pl.ds(pl.multiple_of(p * SEQS + g * 8, 8), 8)
                keys[b, head, rows, :] = kept[p]
            decay_total[b, pl.ds(pl.multiple_of(g * 8, 8), 8), low:high] = running
            scores = dot(jnp.concatenate(products, axis=0).astype(BF16), ones)
            number = 0
            for p in range(SLOTS):
                read = None
                for value in values[: p + 1]:
                    term = scores[number * 8 : (number + 1) * 8] * value
                    read = term if read is None else read + term
                    number += 1
                own_read[head, pl.ds(pl.multiple_of(p * SEQS + g * 8, 8), 8), :] = read
        return carry

    lax.fori_loop(0, (SEQS // 8 - done) // together, group, 0)


def reads(b, head, lo, refs):
    spread, rounded, gain, q_decayed, own_read, heads_out = refs
    together = 8
    low, high = head * LANES, (head + 1) * LANES

    def group(g, carry):
        for unit in range(together):
            s = g * together + unit
            rows = pl.ds(s, SLOTS, stride=SEQS)
            read = dot(q_decayed[head, rows, :].astype(BF16), rounded[s, head])
            read = read + own_read[head, rows, :]
            square = jnp.mean(read * read, axis=1, keepdims=True)
            gate = silu(spread[b, head, 3, rows, :])
            out = read * lax.rsqrt(square + EPSILON) * gain[b : b + 1, low:high] * gate
            heads_out[head, pl.ds(pl.multiple_of(s * SLOTS, SLOTS), SLOTS), :] = out
        return carry

    lax.fori_loop(lo // SLOTS // together, SEQS // together, group, 0)


def round_states(b, states, rounded):
    def group(g, carry):
        rounded[pl.ds(g * 4, 4)] = states[b, pl.ds(g * 4, 4)].astype(BF16)
        return carry

    lax.fori_loop(0, SEQS // 4, group, 0)


def advance_states(b, first, number, refs):
    states, spread, keys, decay_total = refs

    def group(g, carry):
        diagonal = iota((LANES, LANES), 0) == iota((LANES, LANES), 1)
        totals = decay_total[b, pl.ds(pl.multiple_of(g * 8, 8), 8), :]
        for unit in range(8):
            s = g * 8 + unit
            slots = pl.ds(s, SLOTS, stride=SEQS)
            for head in range(HEADS):
                added = dot_rows(
                    keys[b, head, slots, :].astype(BF16), spread[b, head, 2, slots, :].astype(BF16)
                )
                total = totals[unit : unit + 1, head * LANES : (head + 1) * LANES]
                kept = jnp.sum(jnp.where(diagonal, total, 0.0), axis=1, keepdims=True)
                states[b, s, head] = kept * states[b, s, head] + added
        return carry

    lax.fori_loop(first, first + number, group, 0)


def blocks_kernel(pieces, *refs):
    count = len(pieces)
    (spans, act, gain_in, w_q, w_f, w_v, w_g, minimum, extra, gain_out, emission, memory) = refs[:12]
    (rank, many, final_x, states) = refs[12:16]
    refs = list(refs[16:])

    def take(number):
        taken = refs[:number]
        del refs[:number]
        return taken

    (gathered, column, raw, gain_peer, weights, outward, rounded, normed, spread, q_decayed, own_read) = take(11)
    (heads_out, added, keys, decay_total) = take(4)
    (local_sems, swap_send, swap_recv, count_send, count_recv, send_sems, recv_sems) = take(7)
    per = [take(13) for _ in range(count)]
    x, core, z, y = here()
    dp = x * 2 + core

    xs = [device(around(x, o), core, z, y) for o in range(1, RING)]
    ys = [device(x, core, z, around(y, o)) for o in range(1, RING)]
    zs = [device(x, core, around(z, o), y) for o in range(1, RING)]
    crossed = [device(x, 1 - core, around(z, o), y) for o in range(RING)]
    others = [device(around(x, o), 1 - core, z, y) for o in range(1, RING)]
    partner = crossed[0]
    kernels = (w_q, w_f, w_v, w_g)

    local, swaps, sent = [], [], []

    def bring(parts, whole):
        sem = local_sems.at[len(local)]
        for source, target in parts:
            pltpu.make_async_copy(source, target, sem).start()
        local.append(pltpu.make_async_copy(whole, whole, sem))
        return local[-1]

    def swap(parts, whole):
        send_sem, recv_sem = swap_send.at[len(swaps)], swap_recv.at[len(swaps)]
        for source, target in parts:
            pltpu.make_async_remote_copy(
                source, target, send_sem, recv_sem, device_id=partner, device_id_type=MESH
            ).start()
        swaps.append(pltpu.make_async_copy(whole, whole, send_sem))
        return pltpu.make_async_copy(whole, whole, recv_sem)

    def scatter(b, i, phase, number, copies, sources, targets):
        send_sem, recv_sem = send_sems.at[b, i, phase, number], recv_sems.at[b, i, phase, number]
        for source, target, peer in copies:
            pltpu.make_async_remote_copy(
                source, target, send_sem, recv_sem, device_id=peer, device_id_type=MESH
            ).start()
        sent.append(pltpu.make_async_copy(sources, sources, send_sem))
        return pltpu.make_async_copy(targets, targets, recv_sem)

    def rows_of(side, j):
        return act.at[pl.ds((j * 2 + side) * SHARD_ROWS, SHARD_ROWS), :]

    def row_parts(side, low):
        columns = slice(low, low + FEATURES)
        return [(rows_of(side, j), raw.at[j, :, columns]) for j in range(RING)], raw.at[:, :, columns]

    def weight_parts(b, head, low):
        rows = slice(low, low + FEATURES)
        parts = [
            (
                kernels[k].at[b, :, head * LANES : (head + 1) * LANES],
                weights.at[b, head, rows, k * LANES : (k + 1) * LANES],
            )
            for k in range(4)
        ]
        return parts, weights.at[b, head, rows]

    def outward_parts(b, low):
        place = outward.at[b, :, low : low + FEATURES]
        return [(emission.at[b], place)], place

    own_rows = bring(*row_parts(core, 0))
    own_weights = [[bring(*weight_parts(0, head, 0)) for head in range(HEADS)]]

    greet(xs + ys + zs + crossed + others)

    counts = []
    for number, peer in enumerate(xs + [partner] + others):
        copy = pltpu.make_async_remote_copy(
            spans,
            gathered.at[dp],
            count_send.at[number],
            count_recv.at[number],
            device_id=peer,
            device_id_type=MESH,
        )
        copy.start()
        counts.append(copy)
    peer_rows = swap(*row_parts(1 - core, FEATURES))
    peer_gain = swap([(gain_in, gain_peer)], gain_peer)
    peer_weights = [[swap(*weight_parts(0, head, FEATURES)) for head in range(HEADS)]]
    own_states = [bring([(memory.at[b], states.at[b])], states.at[b]) for b in range(BLOCKS)]
    own_outward = [bring(*outward_parts(b, 0)) for b in range(BLOCKS)]
    own_weights.append([bring(*weight_parts(1, head, 0)) for head in range(HEADS)])
    peer_outward = [swap(*outward_parts(b, FEATURES)) for b in range(BLOCKS)]
    peer_weights.append([swap(*weight_parts(1, head, FEATURES)) for head in range(HEADS)])

    gathered[dp] = spans[...]
    fill_columns(spans, column)
    for copy in counts:
        copy.wait_recv()
    fill_ranks(gathered, rank, many)
    own_rows.wait()
    peer_rows.wait()
    peer_gain.wait()
    waiting = []

    def widen():
        diagonal = iota((LANES, LANES), 0) == iota((LANES, LANES), 1)
        for b in range(BLOCKS):
            for head in range(HEADS):
                for part in range(SHARD_ROWS // LANES):
                    row = extra[b, head : head + 1, part * LANES : (part + 1) * LANES]
                    wide = jnp.sum(jnp.where(diagonal, jnp.exp(row), 0.0), axis=1, keepdims=True)
                    added[b, head, part * LANES : (part + 1) * LANES, :] = jnp.broadcast_to(wide, (LANES, LANES))

    def piece_steps(i):
        first, rows = pieces[i]
        (x_own, x_peer, parts, got, squares, got_squares, heads, u_own, u_peer, one, two_own, two_peer, last_peer) = per[i]
        for j in range(RING):
            picked = dot(chosen(rank[j * 2 + core], first, rows), raw[j]).astype(BF16)
            for part in range(CHUNKS):
                x_own[0, part, j] = picked[:, part * WIDE : (part + 1) * WIDE]
                x_peer[0, part, j] = picked[:, FEATURES + part * WIDE : FEATURES + (part + 1) * WIDE]
        for b in range(BLOCKS):
            wide = max(rows, LANES)
            eye = iota((rows, wide), 0) == iota((rows, wide), 1)
            for j in range(RING):
                total = jnp.zeros((rows, 1), F32)
                for part in range(CHUNKS):
                    own = x_own[b, part, j].astype(F32)
                    peer = x_peer[b, part, j].astype(F32)
                    total = total + jnp.sum(own * own + peer * peer, axis=1, keepdims=True)
                squares[b, j] = jnp.sum(jnp.where(eye, total, 0.0), axis=0, keepdims=True)
            square_wait = scatter(
                b, i, 0, 0,
                [(squares.at[b, around(x, o)], got_squares.at[b, o - 1], xs[o - 1]) for o in (2, 1, 3)],
                squares.at[b, 0:3], got_squares.at[b],
            )
            for j in range(RING):
                at = slice(j * rows, (j + 1) * rows)
                for part in range(CHUNKS):
                    low, high = part * WIDE, (part + 1) * WIDE
                    own = x_own[b, part, j].astype(F32) * gain_in[b : b + 1, low:high]
                    peer = x_peer[b, part, j].astype(F32) * gain_peer[b : b + 1, low:high]
                    normed[at, low:high] = own.astype(BF16)
                    normed[at, FEATURES + low : FEATURES + high] = peer.astype(BF16)
            waits = []
            for head in range(HEADS):
                if i == 0:
                    own_weights[b][head].wait()
                    peer_weights[b][head].wait()

                def project(k, carry, b=b, head=head):
                    columns = pl.ds(pl.multiple_of(k * CHANNELS, CHANNELS), CHANNELS)
                    product = dot(normed[0 : RING * rows], weights[b, head, :, columns]).astype(BF16)
                    for j in range(RING):
                        parts[b, head, j, :, columns] = product[j * rows : (j + 1) * rows]
                    return carry

                lax.fori_loop(0, 2, project, 0)
                waits.append(
                    scatter(
                        b, i, 1, head,
                        [(parts.at[b, head, around(x, o)], got.at[b, head, o - 1], xs[o - 1]) for o in (2, 1, 3)],
                        parts.at[b, head, 0:3], got.at[b, head],
                    )
                )
            if i == count - 1:
                if b == 0:
                    widen()
                own_states[b].wait()
                round_states(b, states, rounded)
            yield

            square_wait.wait()
            square = squares[b, x] + got_squares[b, 0] + got_squares[b, 1] + got_squares[b, 2]
            scale_row = lax.rsqrt(square / D + EPSILON)
            scale = jnp.sum(jnp.where(eye, scale_row, 0.0), axis=1, keepdims=True)
            places = chosen(rank[SHARDS + dp], first, rows)
            picking = chosen(rank[dp], first, rows)
            head_waits = []
            for head in range(HEADS):
                waits[head].wait()

                for part in range(2):
                    columns = slice(part * CHANNELS, (part + 1) * CHANNELS)
                    total = parts[b, head, x, :, columns].astype(F32)
                    for o in range(RING - 1):
                        total = total + got[b, head, o, :, columns].astype(F32)
                    placed = dot_rows(places, (total * scale).astype(BF16))
                    for k in range(2):
                        piece = placed[:, k * LANES : (k + 1) * LANES]
                        if i > 0:
                            piece = piece + spread[b, head, part * 2 + k]
                        spread[b, head, part * 2 + k] = piece
                gates(b, head, first, first + rows, (spread, column, minimum, added, q_decayed, own_read, keys, decay_total))
                reads(b, head, first, (spread, rounded, gain_out, q_decayed, own_read, heads_out))
                heads[b, head, x] = dot(picking, heads_out[head].astype(BF16)).astype(BF16)
                mine, three = heads.at[b, head, x], heads.at[b, head, 0:3]
                head_waits.append(
                    scatter(b, i, 2, head, [(mine, mine, xs[o - 1]) for o in (2, 1, 3)], three, three)
                )
            if i == count - 1:
                for g in range(SEQS // 8):
                    waiting.append(
                        functools.partial(advance_states, b, g, 1, (states, spread, keys, decay_total))
                    )
            if i == 0:
                own_outward[b].wait()
                peer_outward[b].wait()
            yield

            for wait in head_waits:
                wait.wait()
            all_heads = jnp.concatenate([heads[b, head].reshape(RING * rows, LANES) for head in range(HEADS)], axis=1)
            waits = []
            for part in range(CHUNKS):
                for half, (target, at, peers) in enumerate(((u_own, y, ys), (u_peer, z, zs))):
                    low = half * FEATURES + part * WIDE
                    product = dot(all_heads, outward[b, :, low : low + WIDE]).astype(BF16)
                    for j in range(RING):
                        target[b, part, j] = product[j * rows : (j + 1) * rows]
                    waits.append(
                        scatter(
                            b, i, 3 + half, part,
                            [
                                (target.at[b, part, around(at, o)], one.at[b, half, part, o - 1], peers[o - 1])
                                for o in (2, 1, 3)
                            ],
                            target.at[b, part, 0:3], one.at[b, half, part],
                        )
                    )
            yield

            later = []
            for part in range(CHUNKS):
                for half, (mine, at, slots, own, peers) in enumerate(
                    ((u_own, y, two_own, z, zs), (u_peer, z, two_peer, y, ys))
                ):
                    waits.pop(0).wait()
                    total = mine[b, part, at].astype(F32)
                    for o in range(RING - 1):
                        total = total + one[b, half, part, o].astype(F32)
                    slots[b, part, own] = total.astype(BF16)
                    place, three = slots.at[b, part, own], slots.at[b, part, 0:3]
                    later.append(
                        scatter(b, i, 5 + half, part, [(place, place, peers[o - 1]) for o in (2, 1, 3)], three, three)
                    )
            waits = later
            yield

            later = []
            for part in range(CHUNKS):
                for half, (slots, old, at) in enumerate(((two_own, x_own, y), (two_peer, x_peer, z))):
                    waits.pop(0).wait()
                    total = slots[b, part, 0].astype(F32)
                    for o in range(1, RING):
                        total = total + slots[b, part, o].astype(F32)
                    fresh = (old[b, part, at].astype(F32) + total.astype(BF16).astype(F32)).astype(BF16)
                    within = slice(first, first + rows)
                    if b < BLOCKS - 1:
                        old[b + 1, part, at] = fresh
                        place, three = old.at[b + 1, part, at], old.at[b + 1, part, 0:3]
                        peers = ys if half == 0 else zs
                        copies = [(place, place, peers[o - 1]) for o in (2, 1, 3)]
                        later.append(scatter(b, i, 7 + half, part, copies, three, three))
                    elif half == 0:
                        final_x[core, part, y, within] = fresh
                        place, three = final_x.at[core, part, y, within], final_x.at[core, part, 0:3, within]
                        copies = [(place, place, ys[o - 1]) for o in (2, 1, 3)]
                        later.append(scatter(b, i, 7, part, copies, three, three))
                    else:
                        last_peer[part] = fresh
                        place, four = final_x.at[core, part, z, within], final_x.at[1 - core, part, 0:4, within]
                        copies = [(last_peer.at[part], place, crossed[o]) for o in (2, 1, 3, 0)]
                        later.append(scatter(b, i, 8, part, copies, four, four))
            yield
            for wait in later:
                wait.wait()

    running = [piece_steps(i) for i in range(count)]
    tick, aged = 0, []
    while running:
        still = []
        for steps in running:
            try:
                next(steps)
                still.append(steps)
            except StopIteration:
                pass
            for _ in range(ADVANCES.get((tick % 5, steps is running[-1]), 0)):
                if waiting:
                    waiting.pop(0)()
        for copy in aged:
            copy.wait()
        aged = list(sent)
        sent.clear()
        if tick == 1:
            for copy in swaps:
                copy.wait()
            for copy in counts:
                copy.wait_send()
        running = still
        tick += 1

    for work in waiting:
        work()
    for copy in aged + sent:
        copy.wait()


def blocks(pieces, *args):
    capacity = sum(rows for _, rows in pieces)
    hbm = pl.BlockSpec(memory_space=pltpu.HBM)
    vmem = pl.BlockSpec(memory_space=pltpu.VMEM)
    scratch = [
        pltpu.VMEM((SHARDS, 1, SEQS), jnp.int32),
        pltpu.VMEM((2 * SEQS, LANES), F32),
        pltpu.VMEM((RING, SHARD_ROWS, 2 * FEATURES), BF16),
        pltpu.VMEM((BLOCKS, FEATURES), F32),
        pltpu.VMEM((BLOCKS, HEADS, 2 * FEATURES, 4 * LANES), BF16),
        pltpu.VMEM((BLOCKS, CHANNELS, 2 * FEATURES), BF16),
        pltpu.VMEM((SEQS, HEADS, LANES, LANES), BF16),
        pltpu.VMEM((RING * max(rows for _, rows in pieces), 2 * FEATURES), BF16),
        pltpu.VMEM((BLOCKS, HEADS, 4, SHARD_ROWS, LANES), F32),
        pltpu.VMEM((HEADS, SHARD_ROWS, LANES), F32),
        pltpu.VMEM((HEADS, SHARD_ROWS, LANES), F32),
        pltpu.VMEM((HEADS, SHARD_ROWS, LANES), F32),
        pltpu.VMEM((BLOCKS, HEADS, SHARD_ROWS, LANES), F32),
        pltpu.VMEM((BLOCKS, HEADS, SHARD_ROWS, LANES), F32),
        pltpu.VMEM((BLOCKS, SEQS, CHANNELS), F32),
        pltpu.SemaphoreType.DMA((9,)),
        pltpu.SemaphoreType.DMA((8,)),
        pltpu.SemaphoreType.DMA((8,)),
        pltpu.SemaphoreType.DMA((SHARDS - 1,)),
        pltpu.SemaphoreType.DMA((SHARDS - 1,)),
        pltpu.SemaphoreType.DMA((BLOCKS, len(pieces), 9, max(HEADS, CHUNKS))),
        pltpu.SemaphoreType.DMA((BLOCKS, len(pieces), 9, max(HEADS, CHUNKS))),
    ]
    for _, rows in pieces:
        scratch += [
            pltpu.VMEM((BLOCKS, CHUNKS, RING, rows, WIDE), BF16),
            pltpu.VMEM((BLOCKS, CHUNKS, RING, rows, WIDE), BF16),
            pltpu.VMEM((BLOCKS, HEADS, RING, rows, 4 * LANES), BF16),
            pltpu.VMEM((BLOCKS, HEADS, RING - 1, rows, 4 * LANES), BF16),
            pltpu.VMEM((BLOCKS, RING, 1, max(rows, LANES)), F32),
            pltpu.VMEM((BLOCKS, RING - 1, 1, max(rows, LANES)), F32),
            pltpu.VMEM((BLOCKS, HEADS, RING, rows, LANES), BF16),
            pltpu.VMEM((BLOCKS, CHUNKS, RING, rows, WIDE), BF16),
            pltpu.VMEM((BLOCKS, CHUNKS, RING, rows, WIDE), BF16),
            pltpu.VMEM((BLOCKS, 2, CHUNKS, RING - 1, rows, WIDE), BF16),
            pltpu.VMEM((BLOCKS, CHUNKS, RING, rows, WIDE), BF16),
            pltpu.VMEM((BLOCKS, CHUNKS, RING, rows, WIDE), BF16),
            pltpu.VMEM((CHUNKS, rows, WIDE), BF16),
        ]
    return pl.pallas_call(
        functools.partial(blocks_kernel, pieces),
        out_shape=(
            jax.ShapeDtypeStruct((2 * SHARDS, 1, SHARD_ROWS), F32),
            jax.ShapeDtypeStruct((1, 1), jnp.int32),
            jax.ShapeDtypeStruct((2, CHUNKS, RING, capacity, WIDE), BF16),
            pltpu.VMEM((BLOCKS, SEQS, HEADS, LANES, LANES), F32),
        ),
        in_specs=[vmem, hbm, vmem] + [hbm] * 4 + [vmem] * 3 + [hbm] * 2,
        out_specs=(vmem, pl.BlockSpec(memory_space=pltpu.SMEM), vmem, vmem),
        scratch_shapes=scratch,
        compiler_params=pltpu.CompilerParams(
            collective_id=len(pieces) + capacity, has_side_effects=True, vmem_limit_bytes=(32 if capacity == CAPACITY else 44) * MIB
        ),
        name="blocks",
    )(*args)


def outputs_kernel(rank, rows, held, act, mixed, states, old, fresh, state_sems, in_sems, out_sems):
    capacity = rows.shape[3]
    shard_rows = [pl.ds(d * SHARD_ROWS, SHARD_ROWS) for d in range(SHARDS)]
    loads = [pltpu.make_async_copy(act.at[shard_rows[d]], old.at[d], in_sems.at[d]) for d in range(SHARDS)]
    for load in loads:
        load.start()
    writes = [pltpu.make_async_copy(held.at[b], states.at[b], state_sems.at[b]) for b in range(BLOCKS)]
    for write in writes:
        write.start()
    def write_rows(d):
        place = mixed.at[pl.ds(pl.multiple_of(d * SHARD_ROWS, SHARD_ROWS), SHARD_ROWS)]
        return pltpu.make_async_copy(fresh.at[d], place, out_sems.at[d])

    for load in loads:
        load.wait()

    def shard(d, carry):
        places = chosen(rank[d], 0, capacity)
        live = dot_rows(places, jnp.ones((capacity, LANES), BF16)) > 0.5
        for chunk in range(CHUNKS):
            spread = dot_rows(places, rows[lax.rem(d, 2), chunk, lax.div(d, 2)]).astype(BF16)
            for part in range(WIDE // LANES):
                low = chunk * WIDE + part * LANES
                fresh[d, :, low : low + LANES] = jnp.where(
                    live, spread[:, part * LANES : (part + 1) * LANES], old[d, :, low : low + LANES]
                )
        write_rows(d).start()
        return carry

    lax.fori_loop(0, SHARDS, shard, 0)
    for d in range(SHARDS):
        write_rows(d).wait()
    for write in writes:
        write.wait()


def write_out(rank, rows, held, act):
    anywhere = pl.BlockSpec(memory_space=pl.ANY)
    vmem = pl.BlockSpec(memory_space=pltpu.VMEM)
    return pl.pallas_call(
        outputs_kernel,
        out_shape=(
            jax.ShapeDtypeStruct(act.shape, BF16),
            jax.ShapeDtypeStruct(held.shape, F32),
        ),
        in_specs=[vmem, vmem, vmem, anywhere],
        out_specs=(anywhere, anywhere),
        scratch_shapes=[
            pltpu.VMEM((SHARDS, SHARD_ROWS, FEATURES), BF16),
            pltpu.VMEM((SHARDS, SHARD_ROWS, FEATURES), BF16),
            pltpu.SemaphoreType.DMA((BLOCKS,)),
            pltpu.SemaphoreType.DMA((SHARDS,)),
            pltpu.SemaphoreType.DMA((SHARDS,)),
        ],
        compiler_params=pltpu.CompilerParams(vmem_limit_bytes=16 * 1024 * 1024),
        name="write_out",
    )(rank, rows, held, act)


CAPACITY = 128
FEW = ((0, 64), (64, 64))
ALL = ((0, 256),)


def local(
    activation_rows,
    fresh_spans,
    entry_rescale_vector,
    probe_kernel,
    retention_kernel,
    content_kernel,
    valve_kernel,
    retention_minimum,
    extra_attenuation,
    channel_rescale_vector,
    emission_kernel,
    memory_grids,
):
    given = (
        fresh_spans.reshape(1, SEQS),
        activation_rows,
        entry_rescale_vector,
        probe_kernel,
        retention_kernel,
        content_kernel,
        valve_kernel,
        retention_minimum,
        jnp.transpose(extra_attenuation, (0, 2, 1)),
        channel_rescale_vector,
        emission_kernel,
        memory_grids,
    )
    rank, many, rows, held = blocks(FEW, *given)
    mixed, states = write_out(rank, rows, held, activation_rows)

    def again(carry):
        rank, _, rows, held = blocks(ALL, *given)
        return (jnp.zeros((), jnp.int32), *write_out(rank, rows, held, activation_rows))

    _, mixed, states = lax.while_loop(lambda carry: carry[0] > 0, again, (many[0, 0], mixed, states))
    return mixed, states


def solution(mesh):
    placed = (
        P(None, "dp"),
        P("dp"),
        P(None, "dp"),
        P(None, "dp", "tp"),
        P(None, "dp", "tp"),
        P(None, "dp", "tp"),
        P(None, "dp", "tp"),
        P(None, "tp"),
        P(None, "dp", "tp"),
        P(None, "tp"),
        P(None, "tp", "dp"),
        P(None, "dp", "tp", None, None),
    )
    return jax.shard_map(
        local,
        mesh=mesh,
        in_specs=placed,
        out_specs=(P(None, "dp"), P(None, "dp", "tp", None, None)),
        check_vma=False,
    )
```
